32 devices in a mesh: sp: 8 (over z, y), tp: 4 (over x, core).
Axes of the slice: x: 2, y: 2, z: 4, core: 2. Of those that a mesh axis runs over, the one named last changes fastest.
Arguments:
- tokens: bfloat16 [8192, 2048], P('sp', 'tp'), may hold values from -6 to 6
- input_norm_gain: float32 [2048], replicated, may hold values from 0.1 to 1.9
- pooling_input_matrix: bfloat16 [2048, 512], P(None, 'tp'), may hold values from -0.125 to 0.125
- query_projection_matrix: bfloat16 [2048, 1024], P(None, 'tp'), may hold values from -0.125 to 0.125
- key_projection_matrix: bfloat16 [2048, 1024], P(None, 'tp'), may hold values from -0.125 to 0.125
- value_projection_matrix: bfloat16 [2048, 1024], P(None, 'tp'), may hold values from -0.125 to 0.125
- output_gate_matrix: bfloat16 [2048, 1024], P(None, 'tp'), may hold values from -0.125 to 0.125
- input_gate_matrix: bfloat16 [2048, 2, 8], replicated
- forget_gate_matrix: bfloat16 [2048, 2, 8], replicated, may hold values from -0.125 to 0.125
- forget_gate_bias: float32 [2, 8], replicated
- log_forget_scale: float32 [2, 8192], P(None, 'sp'), may hold values from 0.35 to 2.8
- extra_log_forget: float32 [2, 8192], P(None, 'sp'), may hold values from -0.7 to 0, as said below
- starting_memory: float32 [2, 8, 128, 128], P(None, 'tp'), may hold values from -3 to 3
- starting_normalizer: float32 [2, 8, 128], P(None, 'tp'), may hold values from -3 to 3
- starting_log_scale: float32 [2, 8], P(None, 'tp'), may hold values from 2 to 5
- pooling_group_map: bfloat16 [4, 128, 128], replicated, may hold values from -0.5 to 0.5
- pooling_channel_scale: float32 [512], replicated, may hold values from 0.1 to 1.9
- memory_head_gain: float32 [1024], replicated, may hold values from 0.1 to 1.9
- pooling_output_matrix: bfloat16 [512, 2048], replicated, may hold values from -0.25 to 0.25
- memory_output_matrix: bfloat16 [1024, 2048], replicated, may hold values from -0.1875 to 0.1875
Outputs:
- mixed_out: bfloat16 [8192, 2048], P(('sp', 'tp'))
The draws below stay inside these ranges and needn't reach their ends.
Inputs may be any that keep to these rules, and one draw needn't show every extreme that they name: `extra_log_forget`: at most three nonzero entries in each direction.
All inputs are finite; a program needn't handle non-finite values.
Results may differ from the reference program's by a relative error of at most 0.0091.
Values may be sent and summed in bfloat16 or wider, within the bound.
A program may use at most 128 MiB of HBM per device.

```python
import jax
import jax.numpy as jnp
from jax import lax

D = 2048
POOL_GROUPS = 4
GROUP_DIM = 128
HEADS = 8
DH = 128
BLOCK = 128
TOK_DEV = 1024
POOL_W = 512
MEM_W = 1024
TOKENS = 8192


def draw_forget_gate_bias(key, part):
    pick_key, slow_key, fast_key = jax.random.split(key, 3)
    slow_share = 0.5
    slow_heads = jax.random.uniform(pick_key, (2, HEADS)) < slow_share
    slow_bias = jnp.log(jnp.float32(TOKENS)) + jax.random.uniform(slow_key, (2, HEADS), minval=1.5, maxval=2.5)
    fast_bias = jax.random.uniform(fast_key, (2, HEADS), minval=3.8, maxval=4.8)
    return jnp.where(slow_heads, slow_bias, fast_bias).astype(jnp.float32)


def draw_log_forget_scale(key, part):
    block_key, rough_key = jax.random.split(key)
    segments = TOKENS // TOK_DEV
    block_factor = jnp.exp(jax.random.uniform(block_key, (2, segments, 1), minval=-0.69, maxval=0.69))
    rough_factor = jax.random.uniform(rough_key, (2, segments, TOK_DEV), minval=0.7, maxval=1.4)
    return (block_factor * rough_factor).reshape(2, TOKENS).astype(jnp.float32)


def draw_extra_log_forget(key, part):
    first_key, second_key, depth_key = jax.random.split(key, 3)
    first_places = jax.random.permutation(first_key, TOKENS)[:3]
    second_places = jax.random.permutation(second_key, TOKENS)[:3]
    places = jnp.stack([first_places, second_places]).astype(jnp.int32)
    depths = jnp.log(jax.random.uniform(depth_key, (2, 3), minval=0.5, maxval=0.8))
    direction_rows = jnp.arange(2)[:, None]
    return jnp.zeros((2, TOKENS), jnp.float32).at[direction_rows, places].set(depths)


def draw_input_gate_matrix(key, part):
    base_key = jax.random.fold_in(key, 0)
    weights = jax.random.normal(base_key, (D, 2, HEADS), jnp.float32) * D ** (-0.5)
    return weights.astype(jnp.bfloat16)


def block_levels(own_key, extent, cuts, smallest, top_value):
    def one(dim, parts):
        steps = jax.random.uniform(jax.random.fold_in(jax.random.fold_in(own_key, 6), dim), (parts,), jnp.float32, smallest / len(cuts), top_value / len(cuts))
        return jnp.repeat(jnp.exp(steps), extent[dim] // parts).reshape((-1,) + (1,) * (len(extent) - dim - 1))

    factor_of = one(*cuts[0])
    for cut in cuts[1:]:
        factor_of = factor_of * one(*cut)
    return factor_of


def gaussian(own_key, dims, deviation, bound, cuts=(), kind=jnp.bfloat16):
    array = jax.random.normal(own_key, dims, jnp.float32) * deviation
    if len(cuts) > 0:
        array = block_levels(own_key, dims, cuts, -0.22, 0.18) * array
    return jnp.clip(array, min=-bound, max=bound).astype(kind)


def setup_inputs(seed: int = 0) -> dict:
    keys = jax.random.split(jax.random.key(seed), 21)
    return {
        "tokens": gaussian(keys[0], (TOKENS, D), 1.0, 6.0, ((0, 8), (1, 4))),
        "input_norm_gain": jnp.clip(1.0 + 0.18 * jax.random.normal(keys[1], (D,), jnp.float32), 0.1, 1.9),
        "pooling_input_matrix": gaussian(keys[2], (D, POOL_W), D ** -0.5, 0.125, ((1, 4),)),
        "query_projection_matrix": gaussian(keys[3], (D, MEM_W), D ** -0.5, 0.125, ((1, 4),)),
        "key_projection_matrix": gaussian(keys[4], (D, MEM_W), D ** -0.5, 0.125, ((1, 4),)),
        "value_projection_matrix": gaussian(keys[5], (D, MEM_W), D ** -0.5, 0.125, ((1, 4),)),
        "output_gate_matrix": gaussian(keys[6], (D, MEM_W), D ** -0.5, 0.125, ((1, 4),)),
        "input_gate_matrix": draw_input_gate_matrix(jax.random.fold_in(keys[20], 71), 0),
        "forget_gate_matrix": gaussian(keys[8], (D, 2, HEADS), D ** -0.5, 0.125),
        "forget_gate_bias": draw_forget_gate_bias(jax.random.fold_in(keys[20], 71), 0),
        "log_forget_scale": draw_log_forget_scale(jax.random.fold_in(keys[20], 71), 0),
        "extra_log_forget": draw_extra_log_forget(jax.random.fold_in(keys[20], 71), 0),
        "starting_memory": gaussian(keys[12], (2, HEADS, DH, DH), 0.5, 3.0, ((1, 4),), jnp.float32),
        "starting_normalizer": gaussian(keys[13], (2, HEADS, DH), 0.5, 3.0, ((1, 4),), jnp.float32),
        "starting_log_scale": jnp.clip(2.0 + 3.0 * jax.random.uniform(keys[14], (2, HEADS), jnp.float32) ** block_levels(keys[14], (2, HEADS), ((1, 4),), -0.2, 0.2), 2.0, 5.0),
        "pooling_group_map": gaussian(keys[15], (POOL_GROUPS, GROUP_DIM, GROUP_DIM), GROUP_DIM ** -0.5, 0.5),
        "pooling_channel_scale": jnp.clip(1.0 + 0.18 * jax.random.normal(keys[16], (POOL_W,), jnp.float32), 0.1, 1.9),
        "memory_head_gain": jnp.clip(1.0 + 0.18 * jax.random.normal(keys[17], (MEM_W,), jnp.float32), 0.1, 1.9),
        "pooling_output_matrix": gaussian(keys[18], (POOL_W, D), POOL_W ** -0.5, 0.25),
        "memory_output_matrix": gaussian(keys[19], (MEM_W, D), MEM_W ** -0.5, 0.1875),
    }


NEG_BIG = -1e+30
LN_EPS = 1e-05
HEAD_EPS = 1e-06
HIGHEST = lax.Precision.HIGHEST

def block_step(carried, pieces):
    memory, normer, maxlog = carried
    q_blk, k_blk, v_blk, i_blk, f_blk = pieces
    lower_mask = jnp.tril(jnp.ones((BLOCK, BLOCK), dtype=bool))
    cumulative = jnp.cumsum(f_blk, axis=-1)
    exponent = jnp.where(lower_mask, cumulative[:, :, None] - cumulative[:, None, :] + i_blk[:, None, :], NEG_BIG)
    carried_log = cumulative + maxlog[:, None]
    row_max = jnp.maximum(carried_log, exponent.max(-1))
    fading = jnp.exp(carried_log - row_max)
    scores = jnp.einsum('htd,hsd->hts', q_blk, k_blk, precision=HIGHEST) * jnp.exp(exponent - row_max[:, :, None])
    numerator = fading[:, :, None] * jnp.einsum('hvk,htk->htv', memory, q_blk, precision=HIGHEST) + jnp.einsum('hts,hsv->htv', scores, v_blk, precision=HIGHEST)
    denominator = fading * jnp.einsum('hk,htk->ht', normer, q_blk, precision=HIGHEST) + scores.sum(-1)
    summed = cumulative[:, -1]
    weight_log = summed[:, None] - cumulative + i_blk
    new_max = jnp.maximum(summed + maxlog, weight_log.max(-1))
    carry_scale = jnp.exp(summed + maxlog - new_max)
    weights = jnp.exp(weight_log - new_max[:, None])
    memory = carry_scale[:, None, None] * memory + jnp.einsum('hsv,hsk->hvk', v_blk * weights[:, :, None], k_blk, precision=HIGHEST)
    normer = carry_scale[:, None] * normer + jnp.einsum('hs,hsk->hk', weights, k_blk, precision=HIGHEST)
    return ((memory, normer, new_max), (numerator, denominator, row_max))

def to_blocks(source):
    return jnp.moveaxis(source.reshape((source.shape[0], source.shape[1] // BLOCK, BLOCK) + source.shape[2:]), 1, 0)

def from_blocks(source):
    return jnp.moveaxis(source, 0, 1).reshape((source.shape[1], source.shape[0] * source.shape[2]) + source.shape[3:])

def memory_direction(query_heads, key_heads, value_heads, log_in, log_forget_gate, initial):
    finals, outputs = lax.scan(block_step, initial, tuple((to_blocks(member) for member in (query_heads, key_heads, value_heads, log_in, log_forget_gate))))
    numerator, denominator, row_max = (from_blocks(member) for member in outputs)
    return numerator / jnp.maximum(jnp.abs(denominator), 1.0)[:, :, None]

def reference(tokens, input_norm_gain, pooling_input_matrix, query_projection_matrix, key_projection_matrix, value_projection_matrix, output_gate_matrix, input_gate_matrix, forget_gate_matrix, forget_gate_bias, log_forget_scale, extra_log_forget, starting_memory, starting_normalizer, starting_log_scale, pooling_group_map, pooling_channel_scale, memory_head_gain, pooling_output_matrix, memory_output_matrix):
    total_rows = tokens.shape[0]
    model_width = tokens.shape[1]
    floats = tokens.astype(jnp.float32)
    mean_row = lax.optimization_barrier(jnp.sum(floats, axis=1)) / model_width
    square_mean = lax.optimization_barrier(jnp.sum(floats * floats, axis=1)) / model_width
    variance = square_mean - mean_row * mean_row
    normed = ((floats - mean_row[:, None]) * lax.rsqrt(variance + LN_EPS)[:, None] * input_norm_gain).astype(jnp.bfloat16)

    def project(weight):
        return jnp.dot(normed, weight, preferred_element_type=jnp.float32)
    pool_in = project(pooling_input_matrix).astype(jnp.bfloat16)
    queries = project(query_projection_matrix).astype(jnp.bfloat16)
    key_rows = project(key_projection_matrix).astype(jnp.bfloat16)
    value_rows = project(value_projection_matrix).astype(jnp.bfloat16)
    out_gate = project(output_gate_matrix).astype(jnp.bfloat16)
    in_pre = project(input_gate_matrix.reshape(model_width, 2 * HEADS)).reshape(total_rows, 2, HEADS)
    forget_gate_preact = project(forget_gate_matrix.reshape(model_width, 2 * HEADS)).reshape(total_rows, 2, HEADS)
    log_forget_gate = jax.nn.log_sigmoid(forget_gate_preact + forget_gate_bias[None]) * log_forget_scale.T[:, :, None] + extra_log_forget.T[:, :, None]

    def heads_of(source, factor):
        return (source.astype(jnp.float32) * factor).reshape(total_rows, HEADS, DH).transpose(1, 0, 2)
    query_heads = heads_of(queries, 1.0)
    key_heads = heads_of(key_rows, DH ** (-0.5))
    value_heads = heads_of(value_rows, 1.0)
    forward = memory_direction(query_heads, key_heads, value_heads, in_pre[:, 0].T, log_forget_gate[:, 0].T, (starting_memory[0], starting_normalizer[0], starting_log_scale[0]))
    backward = memory_direction(query_heads[:, ::-1], key_heads[:, ::-1], value_heads[:, ::-1], in_pre[:, 1].T[:, ::-1], log_forget_gate[:, 1].T[:, ::-1], (starting_memory[1], starting_normalizer[1], starting_log_scale[1]))
    hidden = forward + backward[:, ::-1]
    head_mean = lax.optimization_barrier(jnp.mean(hidden, axis=-1, keepdims=True))
    head_var = lax.optimization_barrier(jnp.mean(jnp.square(hidden - head_mean), axis=-1, keepdims=True))
    scaled = (hidden - head_mean) * lax.rsqrt(head_var + HEAD_EPS) * memory_head_gain.reshape(HEADS, DH)[:, None, :]
    mem_out = (scaled.transpose(1, 0, 2).reshape(total_rows, HEADS * DH) * jax.nn.sigmoid(out_gate.astype(jnp.float32))).astype(jnp.bfloat16)
    positions = jnp.arange(total_rows, dtype=jnp.int32)
    group_outs = []
    for group_index in range(POOL_GROUPS):
        half_span = 2 ** group_index
        grouped = pool_in[:, group_index * GROUP_DIM:(group_index + 1) * GROUP_DIM].astype(jnp.float32)
        padded = jnp.pad(grouped, ((half_span, half_span), (0, 0)))
        pooled = jnp.zeros_like(grouped)
        for offset in range(-half_span, half_span):
            pooled = pooled + padded[half_span + offset:half_span + offset + total_rows]
        upper_edge = jnp.minimum(positions + half_span, total_rows)
        lower_edge = jnp.maximum(positions - half_span, 0)
        counts = (upper_edge - lower_edge).astype(jnp.float32)
        contrast = (pooled / counts[:, None] - grouped).astype(jnp.bfloat16)
        mapped = jnp.dot(contrast, pooling_group_map[group_index], preferred_element_type=jnp.float32)
        group_outs.append((mapped * pooling_channel_scale[group_index * GROUP_DIM:(group_index + 1) * GROUP_DIM]).astype(jnp.bfloat16))
    pool_out = jnp.concatenate(group_outs, axis=1)
    mixed = jnp.dot(pool_out, pooling_output_matrix, preferred_element_type=jnp.float32) + jnp.dot(mem_out, memory_output_matrix, preferred_element_type=jnp.float32)
    return mixed.astype(jnp.bfloat16)
```

```python
import contextlib
import functools
import types

import jax
import jax.numpy as jnp
from jax import lax
from jax.experimental import pallas as pl
from jax.experimental.pallas import tpu as pltpu
from jax.sharding import PartitionSpec as P

DH = 128
NEG_BIG = -1e30
LN_EPS = 1e-05
HEAD_EPS = 1e-06
RIM = 16
AUG = 144
VMEM = pltpu.VMEM
MESH = pl.DeviceIdType.MESH
F32 = jnp.float32
BF16 = jnp.bfloat16
PROFILE = False
KERNEL_VMEM = 48 * 1024 * 1024
SMALL = (
    "gin", "gfg", "gain", "scale", "extra", "bias", "start_mem", "start_norm", "start_log",
    "map", "pscale", "hgain",
)


def scope(name):
    return jax.named_scope(name) if PROFILE else contextlib.nullcontext()


def scan_lanes(values, combine, neutral, forward_rows):
    lanes = values.shape[1]
    lane = lax.broadcasted_iota(jnp.int32, values.shape, 1)
    forward = lax.broadcasted_iota(jnp.int32, values.shape, 0) < forward_rows
    shift = 1
    while shift < lanes:
        low = jnp.where(lane >= shift, pltpu.roll(values, shift, 1), neutral)
        high = jnp.where(lane < lanes - shift, pltpu.roll(values, lanes - shift, 1), neutral)
        values = combine(values, jnp.where(forward, low, high))
        shift *= 2
    return values


def split_three(values):
    high = values.astype(BF16)
    rest = values - high.astype(F32)
    middle = rest.astype(BF16)
    low = (rest - middle.astype(F32)).astype(BF16)
    return high.astype(F32), middle.astype(F32), low.astype(F32)


def wide(row, lanes):
    return jnp.concatenate([row] * (lanes // row.shape[1]), axis=1)


def layer_kernel(tp_size, sp_size, heads, names, *refs):
    k = types.SimpleNamespace(**dict(zip(names, refs, strict=True)))
    me = lax.axis_index("sp")
    group = lax.axis_index("tp")
    far = lax.rem(group + tp_size // 2, tp_size)
    near = group + 1 - 2 * lax.rem(group, 2)
    diagonal = lax.rem(near + tp_size // 2, tp_size)
    others = (far, diagonal, near)
    rows_total, width = k.tokens.shape
    small_refs = [(getattr(k, name + "_in"), getattr(k, name)) for name in SMALL]
    model_width = width * tp_size
    blocks = tp_size
    size = rows_total // blocks
    half = size // 2
    pairs = 2 * heads
    all_heads = k.gin.shape[1]
    group_dim = k.map.shape[1]
    mem_width = heads * DH
    last = blocks - 1
    odd = lax.rem(me, 2)
    partner = me + 1 - 2 * odd
    strides = [1]
    while strides[-1] * 2 < sp_size:
        strides.append(strides[-1] * 2)
    levels = len(strides)

    def route(level, r):
        stride = strides[level]
        if level == 0:
            return True, partner, True
        if r == 0:
            return me + stride < sp_size, me + stride, me >= stride
        return me >= stride, me - stride, me + stride < sp_size

    def when(condition):
        if condition is True:
            return lambda body: body()
        return pl.when(condition)

    rim_sends = (me + 1 < sp_size, me >= 1)
    rim_recvs = (me >= 1, me + 1 < sp_size)

    barrier = pltpu.get_barrier_semaphore()
    peers = jnp.int32(len(others))
    for other in others:
        pl.semaphore_signal(barrier, inc=1, device_id={"tp": other}, device_id_type=MESH)
    greets = []
    for stride in strides:
        greets += [(me + stride < sp_size, me + stride), (me >= stride, me - stride)]
    for okay, other in greets:
        peers = peers + okay.astype(jnp.int32)

        @pl.when(okay)
        def _():
            pl.semaphore_signal(barrier, inc=1, device_id={"sp": other}, device_id_type=MESH)

    spans = [(b * size, size) for b in range(last)]
    spans += [(last * size, half), (last * size + half, half)]
    token_loads = [
        pltpu.make_async_copy(k.tokens.at[pl.ds(a, n)], k.own.at[pl.ds(a, n)], k.token_sem.at[i])
        for i, (a, n) in enumerate(spans)
    ]
    for load in token_loads:
        load.start()

    def load_group(pairs_of, sems, first=0):
        copies = [
            pltpu.make_async_copy(source, target, sems.at[first + i])
            for i, (source, target) in enumerate(pairs_of)
        ]
        for copy in copies:
            copy.start()
        return copies

    smalls = load_group(small_refs, k.small_sem)
    loads = load_group(
        (
            (k.wp_hbm, k.wpg.at[:, pl.ds(0, group_dim)]),
            (k.wk_hbm, k.wk), (k.wv_hbm, k.wv), (k.wq_hbm, k.wq), (k.wo_hbm, k.wo),
        ),
        k.load_sem,
    )
    for load in smalls[:2]:
        load.wait()

    def own_rows(ref, r):
        mine = ref[r, 0:heads, :].astype(F32)
        for other in range(1, tp_size):
            mine = jnp.where(
                group == other, ref[r, other * heads : (other + 1) * heads, :].astype(F32), mine
            )
        return mine

    gate_rows = jnp.concatenate([own_rows(ref, r) for ref in (k.gin, k.gfg) for r in range(2)], axis=0)
    gate_rows = jnp.concatenate(
        [gate_rows, jnp.zeros((128 - 2 * pairs, model_width), F32)], axis=0
    )
    for n in range(model_width // 128):
        at = slice(n * 128, (n + 1) * 128)
        k.wpg[at, group_dim : group_dim + 128] = jnp.transpose(gate_rows[:, at]).astype(BF16)
    s_at = lax.broadcasted_iota(jnp.int32, (size, size), 0)
    t_at = lax.broadcasted_iota(jnp.int32, (size, size), 1)
    k.sums[:, 0:size] = (s_at <= t_at).astype(F32).astype(BF16)
    k.sums[:, size : 2 * size] = (s_at >= t_at).astype(F32).astype(BF16)

    with scope("barrier"):
        pl.semaphore_wait(barrier, peers)

    def to_tp(source, target, send, recv, other):
        return pltpu.make_async_remote_copy(
            src_ref=source, dst_ref=target, send_sem=send, recv_sem=recv,
            device_id={"tp": other}, device_id_type=MESH,
        )

    def to_sp(source, target, send, recv, other):
        return pltpu.make_async_remote_copy(
            src_ref=source, dst_ref=target, send_sem=send, recv_sem=recv,
            device_id={"sp": other}, device_id_type=MESH,
        )

    to_far, to_near, onward = [], [], []
    for i, (a, n) in enumerate(spans):
        s = pl.ds(a, n)
        to_far.append(to_tp(k.own.at[s], k.held.at[1, s], k.far_send.at[i], k.far_recv.at[i], far))
        to_near.append(to_tp(k.own.at[s], k.held.at[0, s], k.near_send.at[i], k.near_recv.at[i], near))
        onward.append(
            to_tp(k.held.at[1, s], k.held.at[2, s], k.pass_send.at[i], k.pass_recv.at[i], near)
        )
    for i in range(len(spans)):
        token_loads[i].wait()
        to_far[i].start()
    for i in range(len(spans)):
        to_near[i].start()
    mem_rows = [
        (k.wmo_hbm.at[pl.ds((g * heads + h) * DH, DH)], k.wmo.at[h, pl.ds(g * DH, DH)])
        for h in range(heads)
        for g in range(tp_size)
    ]
    late_loads = load_group([(k.wpo_hbm, k.wpo)] + mem_rows, k.late_sem)
    for load in smalls[2:]:
        load.wait()

    bias_lane = lax.broadcasted_iota(jnp.int32, k.bias.shape, 1)
    picked = [
        jnp.sum(jnp.where(bias_lane == group * heads + h, k.bias[...], 0.0), axis=1, keepdims=True)
        for h in range(heads)
    ]
    bias = jnp.concatenate([picked[h][r : r + 1] for r in range(2) for h in range(heads)], axis=0)

    def both_rows(ref, span):
        return jnp.concatenate(
            [jnp.broadcast_to(ref[r : r + 1, span], (heads, size)) for r in range(2)], axis=0
        )

    def normalize(a, n, at):
        rows = slice(a, a + n)
        views = [k.own[rows, :]] + [k.held[slot, rows, :] for slot in range(3)]
        total = jnp.zeros((n, 1), F32)
        square = jnp.zeros((n, 1), F32)
        for view in views:
            part = view.astype(F32)
            total = total + jnp.sum(part, axis=1, keepdims=True)
            square = square + jnp.sum(part * part, axis=1, keepdims=True)
        mean = total / model_width
        inverse = lax.rsqrt(square / model_width - mean * mean + LN_EPS)
        for view, owner in zip(views, (group, near, far, diagonal)):
            columns = pl.ds(pl.multiple_of(owner * width, width), width)
            k.normed[at : at + n, columns] = (
                (view.astype(F32) - mean) * inverse * k.gain[:, columns]
            ).astype(BF16)

    def project(a, n, at, targets):
        x = k.normed[at : at + n, :]
        for weight, target in targets:
            target[a : a + n, :] = jnp.dot(x, weight[...], preferred_element_type=F32).astype(BF16)

    def project_gates(a, n, at):
        x = k.normed[at : at + n, :]
        mixed = jnp.dot(x, k.wpg[...], preferred_element_type=F32)
        k.ext[RIM + a : RIM + a + n, :] = mixed[:, :group_dim].astype(BF16).astype(F32)
        k.gates[:, at : at + n] = jnp.transpose(mixed[:, group_dim:])[: 2 * pairs]

    zero_state = jnp.zeros((AUG, DH), F32)

    def initial(r, h):
        is_first = me == (0 if r == 0 else sp_size - 1)
        begin = jnp.broadcast_to(k.start_log[r : r + 1, h : h + 1], (1, 128))
        level = jnp.where(is_first, begin, NEG_BIG)
        rows = jnp.concatenate(
            [k.start_mem[r, h], jnp.broadcast_to(k.start_norm[r, h : h + 1, :], (AUG - DH, DH))], axis=0
        )
        return jnp.where(is_first, rows, 0.0), level

    def prepare():
        for h in range(heads):
            state, level = initial(0, h)
            k.cur_t[h] = state
            k.cur_s[h : h + 1, :] = level
            k.cur_t[heads + h] = zero_state
            k.cur_s[heads + h : heads + h + 1, :] = jnp.full((1, 128), NEG_BIG, F32)
        k.cur_s[pairs : 2 * pairs, :] = jnp.zeros((pairs, 128), F32)

    def summary(b):
        span = slice(b * size, (b + 1) * size)
        pre = k.gates[pairs : 2 * pairs, :] + bias
        log_sig = jnp.minimum(pre, 0.0) - jnp.log1p(jnp.exp(-jnp.abs(pre)))
        log_fg = log_sig * both_rows(k.scale, span) + both_rows(k.extra, span)
        parts = jnp.concatenate(split_three(log_fg), axis=0).astype(BF16)
        sums = jnp.dot(parts, k.sums[...], preferred_element_type=F32)
        sums = sums[:pairs] + sums[pairs : 2 * pairs] + sums[2 * pairs :]
        falls = jnp.concatenate([sums[:heads, :size], sums[heads:, size:]], axis=0)
        lifted = k.gates[:pairs, :] - falls
        top = jnp.max(lifted, axis=1, keepdims=True)
        sources = lifted + jnp.log(F32(DH ** -0.5))
        k.lifted[...] = lifted
        weights = jnp.exp(sources - top)
        peaks = jnp.broadcast_to(top, (pairs, 128))
        fall = jnp.concatenate(
            [falls[:heads, size - 1 : size], falls[heads:, 0:1]], axis=0
        )
        fall = jnp.broadcast_to(fall, (pairs, 128))
        for h in range(heads):
            cols = slice(h * DH, (h + 1) * DH)
            keys = k.k[span, cols]
            vt = jnp.concatenate(
                [jnp.transpose(k.v[span, cols].astype(F32)), jnp.ones((AUG - DH, size), F32)], axis=0
            )
            k.vt[h] = vt.astype(BF16)
            adds = [
                jnp.dot(
                    (vt * weights[p : p + 1]).astype(BF16), keys, preferred_element_type=F32
                )
                for p in (h, heads + h)
            ]
            p = h
            peak, down = peaks[p : p + 1], fall[p : p + 1]
            level = k.cur_s[p : p + 1, :]
            k.enter_t[0, h] = k.cur_t[p].astype(BF16)
            k.enter_s[0, h : h + 1, :] = level
            k.fcum[b, p : p + 1, :] = k.cur_s[pairs + p : pairs + p + 1, :]
            joint = jnp.maximum(level, peak)
            k.cur_t[p] = jnp.exp(level - joint) * k.cur_t[p] + jnp.exp(peak - joint) * adds[0]
            k.cur_s[p : p + 1, :] = joint + down
            k.cur_s[pairs + p : pairs + p + 1, :] += down
            p = heads + h
            peak, down = peaks[p : p + 1], fall[p : p + 1]
            k.ends[b, p : p + 1, :] = peak
            k.ends[b, pairs + p : pairs + p + 1, :] = down
            late = k.cur_s[p : p + 1, :]
            late_fall = k.cur_s[pairs + p : pairs + p + 1, :]
            if b < last:
                k.adds[h, b] = adds[1]
                early, level = adds[1], peak + down
            else:
                state, level = initial(1, h)
                k.back_t[h, b] = state.astype(BF16)
                k.back_s[b, h : h + 1, :] = level
                joint = jnp.maximum(level, peak)
                early = jnp.exp(level - joint) * state + jnp.exp(peak - joint) * adds[1]
                level = joint + down
                if b > 0:
                    k.back_f[h] = early
                    k.back_s[b - 1, h : h + 1, :] = level
            level = level + late_fall
            joint = jnp.maximum(level, late)
            k.cur_t[p] = jnp.exp(level - joint) * early + jnp.exp(late - joint) * k.cur_t[p]
            k.cur_s[p : p + 1, :] = joint
            k.cur_s[pairs + p : pairs + p + 1, :] = late_fall + down

    def local_block(b):
        span = slice(b * size, (b + 1) * size)
        lifted = k.lifted[...]
        peaks = scan_lanes(lifted, jnp.maximum, NEG_BIG, heads)
        levels_in = jnp.concatenate(
            [wide(k.enter_s[0, 0:heads, :], size), jnp.full((heads, size), NEG_BIG, F32)], axis=0
        )
        peaks = jnp.maximum(peaks, levels_in)
        k.peaks[b, 0:pairs, :] = peaks
        carry = jnp.exp(levels_in[:heads] - peaks[:heads])
        sources = lifted + jnp.log(F32(DH ** -0.5))
        columns = jnp.transpose(
            jnp.concatenate([sources, jnp.zeros((128 - pairs, size), F32)], axis=0)
        )
        for h in range(heads):
            cols = slice(h * DH, (h + 1) * DH)
            queries = k.q[span, cols]
            scores = lax.dot_general(
                k.k[span, cols], queries, (((1,), (1,)), ((), ())), preferred_element_type=F32
            )
            values = k.vt[h]
            before = lax.dot_general(
                k.enter_t[0, h], queries, (((1,), (1,)), ((), ())), preferred_element_type=F32
            )
            for r in range(2):
                p = r * heads + h
                inside = (s_at <= t_at) if r == 0 else (s_at >= t_at)
                weight = jnp.exp(
                    jnp.where(inside, columns[:, p : p + 1] - peaks[p : p + 1], NEG_BIG)
                )
                result = jnp.dot(
                    values, (scores * weight).astype(BF16), preferred_element_type=F32
                )
                if r == 0:
                    result = result + carry[h : h + 1] * before
                k.locals[p, b] = result

    def out_gates(b):
        span = slice(b * size, (b + 1) * size)
        for h in range(heads):
            opened = jnp.transpose(k.o[span, h * DH : (h + 1) * DH].astype(F32))
            gain = k.hgain[:, pl.ds(pl.multiple_of(group * mem_width + h * DH, DH), DH)]
            column = jnp.transpose(jnp.broadcast_to(gain, (128, DH)))
            k.gated[h, b] = wide(column, size) / (1.0 + jnp.exp(-opened))

    with scope("prepare"):
        prepare()
    for b in range(blocks):
        pieces = [i for i, (a, n) in enumerate(spans) if b * size <= a < (b + 1) * size]
        with scope(f"far{b}"):
            for i in pieces:
                to_far[i].wait_recv()
                onward[i].start()
        for i in pieces:
            a, n = spans[i]
            at = a - b * size
            with scope(f"wait{i}"):
                to_near[i].wait_recv()
                onward[i].wait_recv()
            if i == 0:
                for load in loads:
                    load.wait()
            with scope(f"project{i}"):
                normalize(a, n, at)
                project_gates(a, n, at)
                project(a, n, at, ((k.wk, k.k), (k.wv, k.v)))
        if b < last:
            with scope(f"local{b}"):
                project(b * size, size, 0, ((k.wq, k.q), (k.wo, k.o)))
                summary(b)
                local_block(b)
                out_gates(b)
        else:
            with scope(f"summary{b}"):
                summary(b)

    for r in range(2):
        for h in range(heads):
            p = r * heads + h
            k.inc_s[r, h : h + 1, :] = k.cur_s[p : p + 1, :]
            k.inc_s[r, heads + h : heads + h + 1, :] = k.cur_s[pairs + p : pairs + p + 1, :]

    def scalar_copy(level, r):
        return to_sp(
            k.send_s.at[level, r], k.recv_s.at[level, r], k.ss.at[level, r], k.sr.at[level, r],
            route(level, r)[1],
        )

    def state_copy(level, r, h):
        return to_sp(
            k.send_t.at[level, r, h], k.recv_t.at[level, r, h], k.ts.at[level, r, h],
            k.tr.at[level, r, h], route(level, r)[1],
        )

    def ready(slot, level, r):
        okay = route(level, r)[0]
        if slot >= 2:
            okay = jnp.logical_and(okay, route(slot - 1, r)[2])
        if level > slot:
            okay = jnp.logical_and(okay, jnp.logical_not(route(slot, r)[2]))
        return okay

    def send_scalars(slot):
        for r in range(2):
            for level in range(slot, levels if slot > 0 else 1):
                @when(ready(slot, level, r))
                def _():
                    k.send_s[level, r] = k.inc_s[r]
                    scalar_copy(level, r).start()

    def send_state(slot, r, h):
        for level in range(slot, levels if slot > 0 else 1):
            @when(ready(slot, level, r))
            def _():
                k.send_t[level, r, h] = k.cur_t[r * heads + h].astype(BF16)
                state_copy(level, r, h).start()

    def take_scalars(level):
        for r in range(2):
            @when(route(level, r)[2])
            def _():
                scalar_copy(level, r).wait_recv()
                theirs_max = k.recv_s[level, r, 0:heads, :]
                theirs_fall = k.recv_s[level, r, heads : 2 * heads, :]
                own_max = k.inc_s[r, 0:heads, :]
                own_fall = k.inc_s[r, heads : 2 * heads, :]
                if level == 0:
                    early = (odd == 1) if r == 0 else (odd == 0)
                    a = jnp.where(early, theirs_max + own_fall, theirs_max)
                    c = jnp.where(early, own_max, own_max + theirs_fall)
                    flag = jnp.where(early, 1.0, 0.0).astype(F32)
                    k.weigh[r, 2 * heads : 3 * heads, :] = jnp.full((heads, 128), flag, F32)
                    k.exc_s[r, 0:heads, :] = jnp.where(early, theirs_max, NEG_BIG)
                    k.exc_s[r, heads : 2 * heads, :] = jnp.where(early, theirs_fall, 0.0)
                else:
                    a = theirs_max + own_fall
                    c = own_max
                    late_max = k.exc_s[r, 0:heads, :]
                    late_fall = k.exc_s[r, heads : 2 * heads, :]
                    level_in = theirs_max + late_fall
                    top = jnp.maximum(level_in, late_max)
                    k.weigh[r, 2 * heads : 3 * heads, :] = jnp.exp(level_in - top)
                    k.weigh[r, 3 * heads : 4 * heads, :] = jnp.exp(late_max - top)
                    k.exc_s[r, 0:heads, :] = top
                    k.exc_s[r, heads : 2 * heads, :] = theirs_fall + late_fall
                top = jnp.maximum(a, c)
                k.weigh[r, 0:heads, :] = jnp.exp(a - top)
                k.weigh[r, heads : 2 * heads, :] = jnp.exp(c - top)
                k.inc_s[r, 0:heads, :] = top
                k.inc_s[r, heads : 2 * heads, :] = theirs_fall + own_fall

    def take_state(level, r, h):
        @when(route(level, r)[2])
        def _():
            state_copy(level, r, h).wait_recv()
            p = r * heads + h
            arrived = k.recv_t[level, r, h].astype(F32)
            if level + 1 < levels:
                k.cur_t[p] = (
                    k.weigh[r, h : h + 1, :] * arrived
                    + k.weigh[r, heads + h : heads + h + 1, :] * k.cur_t[p]
                )
            mine = k.weigh[r, 2 * heads + h : 2 * heads + h + 1, :] * arrived
            if level > 0:
                mine = mine + k.weigh[r, 3 * heads + h : 3 * heads + h + 1, :] * k.exc_t[p]
            k.exc_t[p] = mine

    def rim(side):
        other = me + 1 if side == 0 else me - 1
        return to_sp(k.rim_out.at[side], k.rims.at[side], k.rs.at[side], k.rr.at[side], other)

    def start_rims():
        k.rim_out[1] = k.ext[RIM : 2 * RIM, :].astype(BF16)
        k.rim_out[0] = k.ext[rows_total : RIM + rows_total, :].astype(BF16)
        for side in range(2):
            @pl.when(rim_sends[side])
            def _():
                rim(side).start()

    def pooling():
        for side in range(2):
            at = 0 if side == 0 else RIM + rows_total

            @pl.when(rim_recvs[side])
            def _():
                rim(side).wait_recv()
                k.ext[at : at + RIM, :] = k.rims[side].astype(F32)

            @pl.when(jnp.logical_not(rim_recvs[side]))
            def _():
                k.ext[at : at + RIM, :] = jnp.zeros((RIM, group_dim), F32)
        half_span = jnp.left_shift(jnp.int32(1), group)
        for n in range(blocks):
            first = n * size
            chunk = k.ext[first : first + size + 2 * RIM, :]
            own = chunk[RIM : RIM + size]
            low = 1
            running = chunk[: size + 2 * RIM - 1] + chunk[1:]
            reach = 1
            while 2 * reach < RIM:
                span = running.shape[0] - 2 * reach
                longer = running[:span] + running[2 * reach :]
                kept = running[reach : reach + span]
                running = jnp.where(half_span > reach, longer, kept)
                low += reach
                reach *= 2
            pooled = running[RIM - low : RIM - low + size]
            position = me * rows_total + first + lax.broadcasted_iota(jnp.int32, own.shape, 0)
            count = jnp.minimum(position + half_span, rows_total * sp_size) - jnp.maximum(
                position - half_span, 0
            )
            contrast = (pooled / count.astype(F32) - own).astype(BF16)
            mapped = jnp.dot(contrast, k.map[group], preferred_element_type=F32)
            scale = k.pscale[:, pl.ds(pl.multiple_of(group * group_dim, group_dim), group_dim)]
            k.pool_out[first : first + size, :] = (mapped * scale).astype(BF16)

    pool_cols = pl.ds(pl.multiple_of(group * group_dim, group_dim), group_dim)

    def rows_of(owner):
        return pl.ds(pl.multiple_of(owner * size, size), size)

    own_cols = pl.ds(pl.multiple_of(group * DH, DH), DH)

    pool_copies = [
        to_tp(k.pool_out.at[rows_of(other)], k.lhs_pool.at[:, pool_cols], k.ps.at[j], k.pr.at[j], other)
        for j, other in enumerate(others)
    ]
    mem_copies = [
        [
            to_tp(
                k.mem_out.at[h, rows_of(other)], k.lhs_mem.at[h, :, own_cols],
                k.ms.at[h, j], k.mr.at[h, j], other,
            )
            for j, other in enumerate(others)
        ]
        for h in range(heads)
    ]

    def start_pool():
        pooling()
        for copy in pool_copies:
            copy.start()

    def pool_product():
        k.lhs_pool[:, pool_cols] = k.pool_out[rows_of(group), :]
        for copy in pool_copies:
            copy.wait_recv()
        for load in late_loads:
            load.wait()
        k.acc[...] = jnp.dot(k.lhs_pool[...], k.wpo[...], preferred_element_type=F32)

    def last_local():
        project(last * size, size, 0, ((k.wq, k.q), (k.wo, k.o)))
        local_block(last)
        out_gates(last)

    def backward_enter():
        for h in range(heads):
            p = heads + h
            fall = k.ends[last, pairs + p : pairs + p + 1, :]
            k.fcum[last, p : p + 1, :] = jnp.zeros((1, 128), F32)
            if blocks > 1:
                state, level = k.back_f[h], k.back_s[last - 1, h : h + 1, :]
            for b in reversed(range(last)):
                k.back_t[h, b] = state.astype(BF16)
                k.fcum[b, p : p + 1, :] = fall
                if b > 0:
                    peak = k.ends[b, p : p + 1, :]
                    down = k.ends[b, pairs + p : pairs + p + 1, :]
                    joint = jnp.maximum(level, peak)
                    state = jnp.exp(level - joint) * state + jnp.exp(peak - joint) * k.adds[h, b]
                    level = joint + down
                    k.back_s[b - 1, h : h + 1, :] = level
                    fall = fall + down
        for b in range(blocks):
            span = slice(b * size, (b + 1) * size)
            for h in range(heads):
                p = heads + h
                level = wide(k.back_s[b, h : h + 1, :], size)
                peak = k.peaks[b, p : p + 1, :]
                joint = jnp.maximum(level, peak)
                before = lax.dot_general(
                    k.back_t[h, b], k.q[span, h * DH : (h + 1) * DH], (((1,), (1,)), ((), ())),
                    preferred_element_type=F32,
                )
                k.locals[p, b] = (
                    jnp.exp(peak - joint) * k.locals[p, b] + jnp.exp(level - joint) * before
                )
                k.peaks[b, p : p + 1, :] = joint

    def finish(b, h):
        states = jnp.concatenate([k.exc_t[h], k.exc_t[heads + h]], axis=0).astype(BF16)
        queries = k.q[rows_of(b), h * DH : (h + 1) * DH]
        entered = lax.dot_general(
            states, queries, (((1,), (1,)), ((), ())), preferred_element_type=F32
        )
        hidden = None
        for r in range(2):
            p = r * heads + h
            level = wide(k.exc_s[r, h : h + 1, :] + k.fcum[b, p : p + 1, :], size)
            peak = k.peaks[b, p : p + 1, :]
            joint = jnp.maximum(level, peak)
            a = jnp.exp(peak - joint)
            c = jnp.exp(level - joint)
            mine = k.locals[p, b]
            theirs = entered[r * AUG : (r + 1) * AUG]
            below = a * mine[DH : DH + 1] + c * theirs[DH : DH + 1]
            inverse = 1.0 / jnp.maximum(jnp.abs(below), 1.0)
            part = (a * inverse) * mine[:DH] + (c * inverse) * theirs[:DH]
            hidden = part if hidden is None else hidden + part
        centered = hidden - jnp.mean(hidden, axis=0, keepdims=True)
        variance = jnp.mean(centered * centered, axis=0, keepdims=True)
        scaled = centered * lax.rsqrt(variance + HEAD_EPS) * k.gated[h, b]
        return jnp.transpose(scaled).astype(BF16)

    with scope("send0"):
        send_scalars(0)
        for h in range(heads):
            for r in range(2):
                send_state(0, r, h)
    for r in range(2):
        for h in range(heads):
            k.exc_t[r * heads + h] = zero_state
    with scope("last_local"):
        start_rims()
        last_local()

    fillers = {0: [("pooling", start_pool)], levels - 1: [("pool_product", pool_product)]}
    fillers.setdefault(max(0, levels - 2), []).append(("backward_enter", backward_enter))
    for level in range(levels):
        final = level + 1 == levels
        if final:
            for name, work in fillers.pop(level, []):
                with scope(name):
                    work()
        with scope(f"scalars{level}"):
            take_scalars(level)
            if not final:
                send_scalars(level + 1)
        for h in range(heads):
            with scope(f"states{level}_{h}"):
                for r in range(2):
                    take_state(level, r, h)
                    if not final:
                        send_state(level + 1, r, h)
            if final:
                with scope(f"finish{h}"):
                    for j, other in enumerate(others):
                        k.mem_out[h, rows_of(other)] = finish(other, h)
                        mem_copies[h][j].start()
                    k.lhs_mem[h, :, own_cols] = finish(group, h)
        if not final:
            for name, work in fillers.pop(level, []):
                with scope(name):
                    work()

    tile = 512
    for h in range(heads):
        with scope(f"wait_mem{h}"):
            for copy in mem_copies[h]:
                copy.wait_recv()
        with scope(f"product{h}"):
            for n in range(model_width // tile):
                cols = slice(n * tile, (n + 1) * tile)
                total = k.acc[:, cols] + jnp.dot(
                    k.lhs_mem[h], k.wmo[h, :, cols], preferred_element_type=F32
                )
                if h + 1 < heads:
                    k.acc[:, cols] = total
                else:
                    k.out[:, cols] = total.astype(BF16)

    for i in range(len(spans)):
        to_far[i].wait_send()
        to_near[i].wait_send()
        onward[i].wait_send()
    for copy in pool_copies + [copy for copies in mem_copies for copy in copies]:
        copy.wait_send()
    for level in range(levels):
        for r in range(2):
            @when(route(level, r)[0])
            def _():
                scalar_copy(level, r).wait_send()
                for h in range(heads):
                    state_copy(level, r, h).wait_send()
    for side in range(2):
        @pl.when(rim_sends[side])
        def _():
            rim(side).wait_send()


def per_device(
    tokens,
    input_norm_gain,
    pooling_input_matrix,
    query_projection_matrix,
    key_projection_matrix,
    value_projection_matrix,
    output_gate_matrix,
    input_gate_matrix,
    forget_gate_matrix,
    forget_gate_bias,
    log_forget_scale,
    extra_log_forget,
    starting_memory,
    starting_normalizer,
    starting_log_scale,
    pooling_group_map,
    pooling_channel_scale,
    memory_head_gain,
    pooling_output_matrix,
    memory_output_matrix,
):
    rows, own_width = tokens.shape
    tp_size = lax.axis_size("tp")
    sp_size = lax.axis_size("sp")
    model_width = own_width * tp_size
    group_dim = pooling_input_matrix.shape[1]
    heads = query_projection_matrix.shape[1] // DH
    mem_width = heads * DH
    pairs = 2 * heads
    levels = max(1, (sp_size - 1).bit_length())
    blocks = tp_size
    size = rows // blocks
    pool_total = pooling_output_matrix.shape[0]
    mem_total = memory_output_matrix.shape[0]
    hbm = pl.BlockSpec(memory_space=pltpu.HBM)
    dma = pltpu.SemaphoreType.DMA
    small = dict(
        gin=input_gate_matrix.transpose(1, 2, 0),
        gfg=forget_gate_matrix.transpose(1, 2, 0),
        gain=input_norm_gain.reshape(1, model_width),
        scale=log_forget_scale,
        extra=extra_log_forget,
        bias=forget_gate_bias,
        start_mem=starting_memory,
        start_norm=starting_normalizer,
        start_log=starting_log_scale,
        map=pooling_group_map,
        pscale=pooling_channel_scale.reshape(1, pool_total),
        hgain=memory_head_gain.reshape(1, mem_total),
    )
    inputs = dict(
        tokens=tokens,
        **{name + "_in": small[name] for name in SMALL},
        wp_hbm=pooling_input_matrix,
        wq_hbm=query_projection_matrix,
        wk_hbm=key_projection_matrix,
        wv_hbm=value_projection_matrix,
        wo_hbm=output_gate_matrix,
        wpo_hbm=pooling_output_matrix,
        wmo_hbm=memory_output_matrix,
    )
    scratch = dict(
        **{name: VMEM(small[name].shape, small[name].dtype) for name in SMALL},
        own=VMEM((rows, own_width), BF16),
        held=VMEM((3, rows, own_width), BF16),
        normed=VMEM((size, model_width), BF16),
        wpg=VMEM((model_width, group_dim + 128), BF16),
        wq=VMEM((model_width, mem_width), BF16),
        wk=VMEM((model_width, mem_width), BF16),
        wv=VMEM((model_width, mem_width), BF16),
        wo=VMEM((model_width, mem_width), BF16),
        wpo=VMEM((pool_total, model_width), BF16),
        wmo=VMEM((heads, tp_size * DH, model_width), BF16),
        lhs_mem=VMEM((heads, size, tp_size * DH), BF16),
        acc=VMEM((size, model_width), F32),
        sums=VMEM((size, 2 * size), BF16),
        ext=VMEM((rows + 2 * RIM, group_dim), F32),
        q=VMEM((rows, mem_width), BF16),
        k=VMEM((rows, mem_width), BF16),
        v=VMEM((rows, mem_width), BF16),
        o=VMEM((rows, mem_width), BF16),
        gates=VMEM((2 * pairs, size), F32),
        lifted=VMEM((pairs, size), F32),
        vt=VMEM((heads, AUG, size), BF16),
        adds=VMEM((heads, blocks, AUG, DH), F32),
        ends=VMEM((blocks, 2 * pairs, 128), F32),
        fcum=VMEM((blocks, pairs, 128), F32),
        peaks=VMEM((blocks, pairs, size), F32),
        locals=VMEM((pairs, blocks, AUG, size), F32),
        gated=VMEM((heads, blocks, DH, size), F32),
        cur_t=VMEM((pairs, AUG, DH), F32),
        cur_s=VMEM((2 * pairs, 128), F32),
        enter_t=VMEM((1, heads, AUG, DH), BF16),
        enter_s=VMEM((1, heads, 128), F32),
        back_t=VMEM((heads, blocks, AUG, DH), BF16),
        back_f=VMEM((heads, AUG, DH), F32),
        back_s=VMEM((blocks, heads, 128), F32),
        inc_s=VMEM((2, 2 * heads, 128), F32),
        exc_t=VMEM((pairs, AUG, DH), F32),
        exc_s=VMEM((2, 2 * heads, 128), F32),
        weigh=VMEM((2, 4 * heads, 128), F32),
        send_t=VMEM((levels, 2, heads, AUG, DH), BF16),
        send_s=VMEM((levels, 2, 2 * heads, 128), F32),
        recv_t=VMEM((levels, 2, heads, AUG, DH), BF16),
        recv_s=VMEM((levels, 2, 2 * heads, 128), F32),
        rim_out=VMEM((2, RIM, group_dim), BF16),
        rims=VMEM((2, RIM, group_dim), BF16),
        pool_out=VMEM((rows, group_dim), BF16),
        mem_out=VMEM((heads, rows, DH), BF16),
        lhs_pool=VMEM((size, pool_total), BF16),
        token_sem=dma((blocks + 1,)),
        load_sem=dma((5,)),
        late_sem=dma((1 + heads * tp_size,)),
        small_sem=dma((len(SMALL),)),
        far_send=dma((blocks + 1,)),
        far_recv=dma((blocks + 1,)),
        near_send=dma((blocks + 1,)),
        near_recv=dma((blocks + 1,)),
        pass_send=dma((blocks + 1,)),
        pass_recv=dma((blocks + 1,)),
        ts=dma((levels, 2, heads)),
        tr=dma((levels, 2, heads)),
        ss=dma((levels, 2)),
        sr=dma((levels, 2)),
        rs=dma((2,)),
        rr=dma((2,)),
        ps=dma((3,)),
        pr=dma((3,)),
        ms=dma((heads, 3)),
        mr=dma((heads, 3)),
    )
    names = tuple(inputs) + ("out",) + tuple(scratch)
    return pl.pallas_call(
        functools.partial(layer_kernel, tp_size, sp_size, heads, names),
        out_shape=VMEM((size, model_width), BF16),
        in_specs=[hbm] * len(inputs),
        out_specs=pl.BlockSpec(memory_space=pltpu.VMEM),
        scratch_shapes=list(scratch.values()),
        compiler_params=pltpu.CompilerParams(
            collective_id=0, has_side_effects=True, vmem_limit_bytes=KERNEL_VMEM
        ),
    )(*(pltpu.with_memory_space_constraint(value, pltpu.HBM) for value in inputs.values()))


def solution(mesh):
    placed = (
        P("sp", "tp"),
        P(),
        P(None, "tp"),
        P(None, "tp"),
        P(None, "tp"),
        P(None, "tp"),
        P(None, "tp"),
        P(),
        P(),
        P(),
        P(None, "sp"),
        P(None, "sp"),
        P(None, "tp", None, None),
        P(None, "tp", None),
        P(None, "tp"),
        P(),
        P(),
        P(),
        P(),
        P(),
    )
    return jax.shard_map(
        per_device, mesh=mesh, in_specs=placed, out_specs=P(("sp", "tp"), None), check_vma=False
    )
```

```python
import contextlib
import functools
import types

import jax
import jax.numpy as jnp
from jax import lax
from jax.experimental import pallas as pl
from jax.experimental.pallas import tpu as pltpu
from jax.sharding import PartitionSpec as P

DH = 128
NEG_BIG = -1e30
LN_EPS = 1e-05
HEAD_EPS = 1e-06
RIM = 16
AUG = 144
VMEM = pltpu.VMEM
MESH = pl.DeviceIdType.MESH
F32 = jnp.float32
BF16 = jnp.bfloat16
PROFILE = False
KERNEL_VMEM = 48 * 1024 * 1024
SMALL = (
    "gin", "gfg", "gain", "scale", "extra", "bias", "start_mem", "start_norm", "start_log",
    "map", "pscale", "hgain",
)


def scope(name):
    return jax.named_scope(name) if PROFILE else contextlib.nullcontext()


def scan_lanes(values, combine, neutral, forward_rows):
    lanes = values.shape[1]
    lane = lax.broadcasted_iota(jnp.int32, values.shape, 1)
    forward = lax.broadcasted_iota(jnp.int32, values.shape, 0) < forward_rows
    shift = 1
    while shift < lanes:
        low = jnp.where(lane >= shift, pltpu.roll(values, shift, 1), neutral)
        high = jnp.where(lane < lanes - shift, pltpu.roll(values, lanes - shift, 1), neutral)
        values = combine(values, jnp.where(forward, low, high))
        shift *= 2
    return values


def split_three(values):
    high = values.astype(BF16)
    rest = values - high.astype(F32)
    middle = rest.astype(BF16)
    low = (rest - middle.astype(F32)).astype(BF16)
    return high.astype(F32), middle.astype(F32), low.astype(F32)


def wide(row, lanes):
    return jnp.concatenate([row] * (lanes // row.shape[1]), axis=1)


def layer_kernel(tp_size, sp_size, heads, names, *refs):
    k = types.SimpleNamespace(**dict(zip(names, refs, strict=True)))
    me = lax.axis_index("sp")
    group = lax.axis_index("tp")
    far = lax.rem(group + tp_size // 2, tp_size)
    near = group + 1 - 2 * lax.rem(group, 2)
    diagonal = lax.rem(near + tp_size // 2, tp_size)
    others = (far, diagonal, near)
    rows_total, width = k.tokens.shape
    small_refs = [(getattr(k, name + "_in"), getattr(k, name)) for name in SMALL]
    model_width = width * tp_size
    blocks = tp_size
    size = rows_total // blocks
    half = size // 2
    pairs = 2 * heads
    all_heads = k.gin.shape[1]
    group_dim = k.map.shape[1]
    mem_width = heads * DH
    last = blocks - 1
    odd = lax.rem(me, 2)
    partner = me + 1 - 2 * odd
    strides = [1]
    while strides[-1] * 2 < sp_size:
        strides.append(strides[-1] * 2)
    levels = len(strides)

    def route(level, r):
        stride = strides[level]
        if level == 0:
            return True, partner, True
        step = stride * (1 - 2 * r)
        target, source = me + step, me - step
        okay = jnp.logical_and(target >= 0, target < sp_size)
        has = jnp.logical_and(source >= 0, source < sp_size)
        return okay, target, has

    late_half = (me >= sp_size // 2).astype(jnp.int32)
    leading = (late_half, 1 - late_half)

    def when(condition):
        if condition is True:
            return lambda body: body()
        return pl.when(condition)

    rim_sends = (me + 1 < sp_size, me >= 1)
    rim_recvs = (me >= 1, me + 1 < sp_size)

    barrier = pltpu.get_barrier_semaphore()
    peers = jnp.int32(len(others))
    for other in others:
        pl.semaphore_signal(barrier, inc=1, device_id={"tp": other}, device_id_type=MESH)
    greets = []
    for stride in strides:
        greets += [(me + stride < sp_size, me + stride), (me >= stride, me - stride)]
    for okay, other in greets:
        peers = peers + okay.astype(jnp.int32)

        @pl.when(okay)
        def _():
            pl.semaphore_signal(barrier, inc=1, device_id={"sp": other}, device_id_type=MESH)

    spans = [(b * size, size) for b in range(last)]
    spans += [(last * size, half), (last * size + half, half)]
    token_loads = [
        pltpu.make_async_copy(k.tokens.at[pl.ds(a, n)], k.own.at[pl.ds(a, n)], k.token_sem.at[i])
        for i, (a, n) in enumerate(((0, size), (size, rows_total - size)))
    ]
    for load in token_loads:
        load.start()

    def load_all(pairs_of, semaphore):
        for source, target in pairs_of:
            pltpu.make_async_copy(source, target, semaphore).start()

    def wait_for(ref, semaphore):
        pltpu.make_async_copy(ref, ref, semaphore).wait()

    smalls = [
        pltpu.make_async_copy(source, target, k.small_sem.at[i])
        for i, (source, target) in enumerate(small_refs)
    ]
    for load in smalls:
        load.start()
    pool_weight = pltpu.make_async_copy(
        k.wp_hbm, k.wpg.at[:, pl.ds(0, group_dim)], k.load_sem.at[0]
    )
    pool_weight.start()
    wk, wv, wq, wo = (k.weights.at[i] for i in range(4))
    load_all(
        ((k.wk_hbm, wk), (k.wv_hbm, wv), (k.wq_hbm, wq), (k.wo_hbm, wo)), k.load_sem.at[1]
    )

    def own_rows(ref, r):
        mine = ref[r, 0:heads, :].astype(F32)
        for other in range(1, tp_size):
            mine = jnp.where(
                group == other, ref[r, other * heads : (other + 1) * heads, :].astype(F32), mine
            )
        return mine

    with scope("barrier"):
        pl.semaphore_wait(barrier, peers)

    def to_tp(source, target, send, recv, other):
        return pltpu.make_async_remote_copy(
            src_ref=source, dst_ref=target, send_sem=send, recv_sem=recv,
            device_id={"tp": other}, device_id_type=MESH,
        )

    def to_sp(source, target, send, recv, other):
        return pltpu.make_async_remote_copy(
            src_ref=source, dst_ref=target, send_sem=send, recv_sem=recv,
            device_id={"sp": other}, device_id_type=MESH,
        )

    to_far, onward = [], []
    to_near = to_tp(k.own, k.held.at[0], k.tp_send, k.near_recv, near)
    for i, (a, n) in enumerate(spans):
        s = pl.ds(a, n)
        to_far.append(to_tp(k.own.at[s], k.held.at[1, s], k.tp_send, k.far_recv.at[i], far))
        onward.append(
            to_tp(k.held.at[1, s], k.held.at[2, s], k.tp_send, k.pass_recv.at[i], near)
        )
    token_loads[0].wait()
    to_far[0].start()
    token_loads[1].wait()
    for copy in to_far[1:]:
        copy.start()
    to_near.start()
    mem_rows = [
        (k.wmo_hbm.at[pl.ds((g * heads + h) * DH, DH)], k.wmo.at[h, pl.ds(g * DH, DH)])
        for h in range(heads)
        for g in range(tp_size)
    ]
    out_weight = pltpu.make_async_copy(k.wpo_hbm, k.wpo, k.load_sem.at[2])
    out_weight.start()
    load_all(mem_rows, k.load_sem.at[3])
    for load in smalls:
        load.wait()

    bias_lane = lax.broadcasted_iota(jnp.int32, k.bias.shape, 1)
    picked = [
        jnp.sum(jnp.where(bias_lane == group * heads + h, k.bias[...], 0.0), axis=1, keepdims=True)
        for h in range(heads)
    ]
    bias = jnp.concatenate([picked[h][r : r + 1] for r in range(2) for h in range(heads)], axis=0)

    s_at = lax.broadcasted_iota(jnp.int32, (size, size), 0)
    t_at = lax.broadcasted_iota(jnp.int32, (size, size), 1)

    def gate_weights():
        gate_rows = jnp.concatenate([own_rows(ref, r) for ref in (k.gin, k.gfg) for r in range(2)], axis=0)
        gate_rows = jnp.concatenate(
            [gate_rows, jnp.zeros((128 - 2 * pairs, model_width), F32)], axis=0
        )
        for n in range(model_width // 128):
            at = slice(n * 128, (n + 1) * 128)
            k.wpg[at, group_dim : group_dim + 128] = jnp.transpose(gate_rows[:, at]).astype(BF16)
        k.sums[:, 0:size] = (s_at <= t_at).astype(F32).astype(BF16)
        k.sums[:, size : 2 * size] = (s_at >= t_at).astype(F32).astype(BF16)

    def both_rows(ref, span):
        return jnp.concatenate(
            [jnp.broadcast_to(ref[r : r + 1, span], (heads, size)) for r in range(2)], axis=0
        )

    def normalize(a, n, at):
        rows = slice(a, a + n)
        views = [k.own[rows, :]] + [k.held[slot, rows, :] for slot in range(3)]
        total = jnp.zeros((n, 1), F32)
        square = jnp.zeros((n, 1), F32)
        for view in views:
            part = view.astype(F32)
            total = total + jnp.sum(part, axis=1, keepdims=True)
            square = square + jnp.sum(part * part, axis=1, keepdims=True)
        mean = total / model_width
        inverse = lax.rsqrt(square / model_width - mean * mean + LN_EPS)
        for view, owner in zip(views, (group, near, far, diagonal)):
            columns = pl.ds(pl.multiple_of(owner * width, width), width)
            k.normed[at : at + n, columns] = (
                (view.astype(F32) - mean) * inverse * k.gain[:, columns]
            ).astype(BF16)

    def project(a, n, at, targets):
        x = k.normed[at : at + n, :]
        for weight, target in targets:
            target[a : a + n, :] = jnp.dot(x, weight[...], preferred_element_type=F32).astype(BF16)

    def project_gates(a, n, at):
        x = k.normed[at : at + n, :]
        mixed = jnp.dot(x, k.wpg[...], preferred_element_type=F32)
        k.ext[RIM + a : RIM + a + n, :] = mixed[:, :group_dim].astype(BF16).astype(F32)
        k.gates[:, at : at + n] = jnp.transpose(mixed[:, group_dim:])[: 2 * pairs]

    zero_state = jnp.zeros((AUG, DH), F32)

    def initial(r, h):
        is_first = me == (0 if r == 0 else sp_size - 1)
        begin = jnp.broadcast_to(k.start_log[r : r + 1, h : h + 1], (1, 128))
        level = jnp.where(is_first, begin, NEG_BIG)
        rows = jnp.concatenate(
            [k.start_mem[r, h], jnp.broadcast_to(k.start_norm[r, h : h + 1, :], (AUG - DH, DH))], axis=0
        )
        return jnp.where(is_first, rows, 0.0), level

    def prepare():
        for h in range(heads):
            state, level = initial(0, h)
            k.cur_t[h] = state
            k.cur_s[h : h + 1, :] = level
            k.cur_t[heads + h] = zero_state
            k.cur_s[heads + h : heads + h + 1, :] = jnp.full((1, 128), NEG_BIG, F32)
        k.cur_s[pairs : 2 * pairs, :] = jnp.zeros((pairs, 128), F32)

    def summary(b):
        span = slice(b * size, (b + 1) * size)
        pre = k.gates[pairs : 2 * pairs, :] + bias
        log_sig = jnp.minimum(pre, 0.0) - jnp.log1p(jnp.exp(-jnp.abs(pre)))
        log_fg = log_sig * both_rows(k.scale, span) + both_rows(k.extra, span)
        parts = jnp.concatenate(split_three(log_fg), axis=0).astype(BF16)
        sums = jnp.dot(parts, k.sums[...], preferred_element_type=F32)
        sums = sums[:pairs] + sums[pairs : 2 * pairs] + sums[2 * pairs :]
        falls = jnp.concatenate([sums[:heads, :size], sums[heads:, size:]], axis=0)
        lifted = k.gates[:pairs, :] - falls
        top = jnp.max(lifted, axis=1, keepdims=True)
        sources = lifted + jnp.log(F32(DH ** -0.5))
        k.lifted[...] = lifted
        weights = jnp.exp(sources - top)
        peaks = jnp.broadcast_to(top, (pairs, 128))
        fall = jnp.concatenate(
            [falls[:heads, size - 1 : size], falls[heads:, 0:1]], axis=0
        )
        fall = jnp.broadcast_to(fall, (pairs, 128))
        for h in range(heads):
            cols = slice(h * DH, (h + 1) * DH)
            keys = k.k[span, cols]
            vt = jnp.concatenate(
                [jnp.transpose(k.v[span, cols].astype(F32)), jnp.ones((AUG - DH, size), F32)], axis=0
            )
            k.vt[h] = vt.astype(BF16)
            adds = [
                jnp.dot(
                    (vt * weights[p : p + 1]).astype(BF16), keys, preferred_element_type=F32
                )
                for p in (h, heads + h)
            ]
            p = h
            peak, down = peaks[p : p + 1], fall[p : p + 1]
            level = k.cur_s[p : p + 1, :]
            k.enter_t[0, h] = k.cur_t[p].astype(BF16)
            k.enter_s[0, h : h + 1, :] = level
            k.fcum[b, p : p + 1, :] = k.cur_s[pairs + p : pairs + p + 1, :]
            joint = jnp.maximum(level, peak)
            k.cur_t[p] = jnp.exp(level - joint) * k.cur_t[p] + jnp.exp(peak - joint) * adds[0]
            k.cur_s[p : p + 1, :] = joint + down
            k.cur_s[pairs + p : pairs + p + 1, :] += down
            p = heads + h
            peak, down = peaks[p : p + 1], fall[p : p + 1]
            k.ends[b, p : p + 1, :] = peak
            k.ends[b, pairs + p : pairs + p + 1, :] = down
            late = k.cur_s[p : p + 1, :]
            late_fall = k.cur_s[pairs + p : pairs + p + 1, :]
            if b < last:
                k.adds[h, b] = adds[1]
                early, level = adds[1], peak + down
            else:
                state, level = initial(1, h)
                k.back_t[h, b] = state.astype(BF16)
                k.back_s[b, h : h + 1, :] = level
                joint = jnp.maximum(level, peak)
                early = jnp.exp(level - joint) * state + jnp.exp(peak - joint) * adds[1]
                level = joint + down
                if b > 0:
                    k.back_f[h] = early
                    k.back_s[b - 1, h : h + 1, :] = level
            level = level + late_fall
            joint = jnp.maximum(level, late)
            k.cur_t[p] = jnp.exp(level - joint) * early + jnp.exp(late - joint) * k.cur_t[p]
            k.cur_s[p : p + 1, :] = joint
            k.cur_s[pairs + p : pairs + p + 1, :] = late_fall + down

    def local_block(b):
        span = slice(b * size, (b + 1) * size)
        lifted = k.lifted[...]
        peaks = scan_lanes(lifted, jnp.maximum, NEG_BIG, heads)
        levels_in = jnp.concatenate(
            [wide(k.enter_s[0, 0:heads, :], size), jnp.full((heads, size), NEG_BIG, F32)], axis=0
        )
        peaks = jnp.maximum(peaks, levels_in)
        k.peaks[b, 0:pairs, :] = peaks
        carry = jnp.exp(levels_in[:heads] - peaks[:heads])
        sources = lifted + jnp.log(F32(DH ** -0.5))
        columns = jnp.transpose(
            jnp.concatenate([sources, jnp.zeros((128 - pairs, size), F32)], axis=0)
        )
        for h in range(heads):
            cols = slice(h * DH, (h + 1) * DH)
            queries = k.q[span, cols]
            scores = lax.dot_general(
                k.k[span, cols], queries, (((1,), (1,)), ((), ())), preferred_element_type=F32
            )
            values = k.vt[h]
            before = lax.dot_general(
                k.enter_t[0, h], queries, (((1,), (1,)), ((), ())), preferred_element_type=F32
            )
            for r in range(2):
                p = r * heads + h
                inside = (s_at <= t_at) if r == 0 else (s_at >= t_at)
                weight = jnp.exp(
                    jnp.where(inside, columns[:, p : p + 1] - peaks[p : p + 1], NEG_BIG)
                )
                result = jnp.dot(
                    values, (scores * weight).astype(BF16), preferred_element_type=F32
                )
                if r == 0:
                    result = result + carry[h : h + 1] * before
                k.locals[p, b] = result

    def out_gates(b):
        span = slice(b * size, (b + 1) * size)
        for h in range(heads):
            opened = jnp.transpose(k.o[span, h * DH : (h + 1) * DH].astype(F32))
            gain = k.hgain[:, pl.ds(pl.multiple_of(group * mem_width + h * DH, DH), DH)]
            column = jnp.transpose(jnp.broadcast_to(gain, (128, DH)))
            k.gated[h, b] = wide(column, size) / (1.0 + jnp.exp(-opened))

    with scope("prepare"):
        gate_weights()
        prepare()
    def rim(side):
        other = me + 1 if side == 0 else me - 1
        return to_sp(k.rim_out.at[side], k.rims.at[side], k.rs.at[side], k.rr.at[side], other)

    def start_rims():
        k.rim_out[1] = k.ext[RIM : 2 * RIM, :].astype(BF16)
        k.rim_out[0] = k.ext[rows_total : RIM + rows_total, :].astype(BF16)
        for side in range(2):
            @pl.when(rim_sends[side])
            def _():
                rim(side).start()

    def pass_on(i):
        to_far[i].wait_recv()
        onward[i].start()

    for b in range(blocks):
        pieces = [i for i, (a, n) in enumerate(spans) if b * size <= a < (b + 1) * size]
        with scope(f"far{b}"):
            for i in pieces[1 if b == last and b > 0 else 0 :]:
                pass_on(i)
        for i in pieces:
            a, n = spans[i]
            at = a - b * size
            if i == 0:
                to_near.wait_recv()
            with scope(f"wait{i}"):
                onward[i].wait_recv()
            if i == 0:
                pool_weight.wait()
                wait_for(k.weights, k.load_sem.at[1])
            with scope(f"project{i}"):
                normalize(a, n, at)
                project_gates(a, n, at)
                project(a, n, at, ((wk, k.k), (wv, k.v)))
        if b == last - 1:
            with scope("far_half"):
                pass_on(last)
        if b < last:
            with scope(f"local{b}"):
                project(b * size, size, 0, ((wq, k.q), (wo, k.o)))
                summary(b)
                local_block(b)
                out_gates(b)
        else:
            with scope(f"summary{b}"):
                start_rims()
                summary(b)

    for r in range(2):
        for h in range(heads):
            p = r * heads + h
            k.inc_s[r, h : h + 1, :] = k.cur_s[p : p + 1, :]
            k.inc_s[r, heads + h : heads + h + 1, :] = k.cur_s[pairs + p : pairs + p + 1, :]

    def scalar_copy(level, r):
        return to_sp(
            k.send_s.at[level, r], k.recv_s.at[level, r], k.ss.at[level, r], k.sr.at[level, r],
            route(level, r)[1],
        )

    def state_copy(level, r, h):
        return to_sp(
            k.send_t.at[level, r, h], k.recv_t.at[level, r, h], k.ts.at[level, r],
            k.tr.at[level, r, h], route(level, r)[1],
        )

    def ready(slot, level, r):
        okay = route(level, r)[0]
        if slot >= 2:
            okay = jnp.logical_and(okay, route(slot - 1, r)[2])
        if level > slot:
            okay = jnp.logical_and(okay, jnp.logical_not(route(slot, r)[2]))
        return okay

    def send_scalars(slot):
        for r in range(2):
            for level in range(slot, levels if slot > 0 else 1):
                @when(ready(slot, level, r))
                def _():
                    k.send_s[level, r] = k.inc_s[r]
                    scalar_copy(level, r).start()

    def send_state(slot, r, h):
        for level in range(slot, levels if slot > 0 else 1):
            @when(ready(slot, level, r))
            def _():
                k.send_t[level, r, h] = k.cur_t[r * heads + h].astype(BF16)
                state_copy(level, r, h).start()

    def take_scalars(level):
        for r in range(2):
            @when(route(level, r)[2])
            def _():
                scalar_copy(level, r).wait_recv()
                theirs_max = k.recv_s[level, r, 0:heads, :]
                theirs_fall = k.recv_s[level, r, heads : 2 * heads, :]
                own_max = k.inc_s[r, 0:heads, :]
                own_fall = k.inc_s[r, heads : 2 * heads, :]
                if level == 0:
                    early = (odd == 1) if r == 0 else (odd == 0)
                    a = jnp.where(early, theirs_max + own_fall, theirs_max)
                    c = jnp.where(early, own_max, own_max + theirs_fall)
                    flag = jnp.where(early, 1.0, 0.0).astype(F32)
                    k.weigh[r, 2 * heads : 3 * heads, :] = jnp.full((heads, 128), flag, F32)
                    k.exc_s[r, 0:heads, :] = jnp.where(early, theirs_max, NEG_BIG)
                    k.exc_s[r, heads : 2 * heads, :] = jnp.where(early, theirs_fall, 0.0)
                else:
                    a = theirs_max + own_fall
                    c = own_max
                    late_max = k.exc_s[r, 0:heads, :]
                    late_fall = k.exc_s[r, heads : 2 * heads, :]
                    level_in = theirs_max + late_fall
                    top = jnp.maximum(level_in, late_max)
                    k.weigh[r, 2 * heads : 3 * heads, :] = jnp.exp(level_in - top)
                    k.weigh[r, 3 * heads : 4 * heads, :] = jnp.exp(late_max - top)
                    k.exc_s[r, 0:heads, :] = top
                    k.exc_s[r, heads : 2 * heads, :] = theirs_fall + late_fall
                top = jnp.maximum(a, c)
                k.weigh[r, 0:heads, :] = jnp.exp(a - top)
                k.weigh[r, heads : 2 * heads, :] = jnp.exp(c - top)
                k.inc_s[r, 0:heads, :] = top
                k.inc_s[r, heads : 2 * heads, :] = theirs_fall + own_fall

    def take_state(level, r, h):
        @when(route(level, r)[2])
        def _():
            state_copy(level, r, h).wait_recv()
            p = r * heads + h
            arrived = k.recv_t[level, r, h].astype(F32)
            if level + 1 < levels:
                k.cur_t[p] = (
                    k.weigh[r, h : h + 1, :] * arrived
                    + k.weigh[r, heads + h : heads + h + 1, :] * k.cur_t[p]
                )
            mine = k.weigh[r, 2 * heads + h : 2 * heads + h + 1, :] * arrived
            if level > 0:
                mine = mine + k.weigh[r, 3 * heads + h : 3 * heads + h + 1, :] * k.exc_t[p]
            k.exc_t[p] = mine

    def pooling():
        for side in range(2):
            at = 0 if side == 0 else RIM + rows_total

            @pl.when(rim_recvs[side])
            def _():
                rim(side).wait_recv()
                k.ext[at : at + RIM, :] = k.rims[side].astype(F32)

            @pl.when(jnp.logical_not(rim_recvs[side]))
            def _():
                k.ext[at : at + RIM, :] = jnp.zeros((RIM, group_dim), F32)
        half_span = jnp.left_shift(jnp.int32(1), group)
        for n in range(blocks):
            first = n * size
            chunk = k.ext[first : first + size + 2 * RIM, :]
            own = chunk[RIM : RIM + size]
            low = 1
            running = chunk[: size + 2 * RIM - 1] + chunk[1:]
            reach = 1
            while 2 * reach < RIM:
                span = running.shape[0] - 2 * reach
                longer = running[:span] + running[2 * reach :]
                kept = running[reach : reach + span]
                running = jnp.where(half_span > reach, longer, kept)
                low += reach
                reach *= 2
            pooled = running[RIM - low : RIM - low + size]
            position = me * rows_total + first + lax.broadcasted_iota(jnp.int32, own.shape, 0)
            count = jnp.minimum(position + half_span, rows_total * sp_size) - jnp.maximum(
                position - half_span, 0
            )
            contrast = (pooled / count.astype(F32) - own).astype(BF16)
            mapped = jnp.dot(contrast, k.map[group], preferred_element_type=F32)
            scale = k.pscale[:, pl.ds(pl.multiple_of(group * group_dim, group_dim), group_dim)]
            k.pool_out[first : first + size, :] = (mapped * scale).astype(BF16)

    pool_cols = pl.ds(pl.multiple_of(group * group_dim, group_dim), group_dim)

    def rows_of(owner):
        return pl.ds(pl.multiple_of(owner * size, size), size)

    own_cols = pl.ds(pl.multiple_of(group * DH, DH), DH)

    pool_copies = [
        to_tp(k.pool_out.at[rows_of(other)], k.lhs_pool.at[:, pool_cols], k.pool_send, k.pr, other)
        for j, other in enumerate(others)
    ]
    mem_copies = [
        [
            to_tp(
                k.mem_out.at[h, rows_of(other)], k.lhs_mem.at[h, :, own_cols],
                k.mem_send, k.mr.at[h], other,
            )
            for j, other in enumerate(others)
        ]
        for h in range(heads)
    ]

    def start_pool():
        pooling()
        for copy in pool_copies:
            copy.start()

    def pool_product():
        k.lhs_pool[:, pool_cols] = k.pool_out[rows_of(group), :]
        wait_for(k.pool_out.at[pl.ds(0, len(others) * size)], k.pr)
        out_weight.wait()
        k.acc[...] = jnp.dot(k.lhs_pool[...], k.wpo[...], preferred_element_type=F32)

    def last_local():
        project(last * size, size, 0, ((wq, k.q), (wo, k.o)))
        local_block(last)
        out_gates(last)

    def backward_enter():
        for h in range(heads):
            p = heads + h
            fall = k.ends[last, pairs + p : pairs + p + 1, :]
            k.fcum[last, p : p + 1, :] = jnp.zeros((1, 128), F32)
            if blocks > 1:
                state, level = k.back_f[h], k.back_s[last - 1, h : h + 1, :]
            for b in reversed(range(last)):
                k.back_t[h, b] = state.astype(BF16)
                k.fcum[b, p : p + 1, :] = fall
                if b > 0:
                    peak = k.ends[b, p : p + 1, :]
                    down = k.ends[b, pairs + p : pairs + p + 1, :]
                    joint = jnp.maximum(level, peak)
                    state = jnp.exp(level - joint) * state + jnp.exp(peak - joint) * k.adds[h, b]
                    level = joint + down
                    k.back_s[b - 1, h : h + 1, :] = level
                    fall = fall + down
        for b in range(blocks):
            span = slice(b * size, (b + 1) * size)
            for h in range(heads):
                p = heads + h
                level = wide(k.back_s[b, h : h + 1, :], size)
                peak = k.peaks[b, p : p + 1, :]
                joint = jnp.maximum(level, peak)
                before = lax.dot_general(
                    k.back_t[h, b], k.q[span, h * DH : (h + 1) * DH], (((1,), (1,)), ((), ())),
                    preferred_element_type=F32,
                )
                k.locals[p, b] = (
                    jnp.exp(peak - joint) * k.locals[p, b] + jnp.exp(level - joint) * before
                )
                k.peaks[b, p : p + 1, :] = joint

    def finish(b, h):
        states = jnp.concatenate([k.exc_t[h], k.exc_t[heads + h]], axis=0).astype(BF16)
        queries = k.q[rows_of(b), h * DH : (h + 1) * DH]
        entered = lax.dot_general(
            states, queries, (((1,), (1,)), ((), ())), preferred_element_type=F32
        )
        hidden = None
        for r in range(2):
            p = r * heads + h
            level = wide(k.exc_s[r, h : h + 1, :] + k.fcum[b, p : p + 1, :], size)
            peak = k.peaks[b, p : p + 1, :]
            joint = jnp.maximum(level, peak)
            a = jnp.exp(peak - joint)
            c = jnp.exp(level - joint)
            mine = k.locals[p, b]
            theirs = entered[r * AUG : (r + 1) * AUG]
            below = a * mine[DH : DH + 1] + c * theirs[DH : DH + 1]
            inverse = 1.0 / jnp.maximum(jnp.abs(below), 1.0)
            part = (a * inverse) * mine[:DH] + (c * inverse) * theirs[:DH]
            hidden = part if hidden is None else hidden + part
        centered = hidden - jnp.mean(hidden, axis=0, keepdims=True)
        variance = jnp.mean(centered * centered, axis=0, keepdims=True)
        scaled = centered * lax.rsqrt(variance + HEAD_EPS) * k.gated[h, b]
        return jnp.transpose(scaled).astype(BF16)

    with scope("send0"):
        send_scalars(0)
        for h in range(heads):
            for r in leading:
                send_state(0, r, h)
    for r in range(2):
        for h in range(heads):
            k.exc_t[r * heads + h] = zero_state
    with scope("last_local"):
        last_local()

    def settle(level):
        for r in range(2):
            @when(route(level, r)[0])
            def _():
                scalar_copy(level, r).wait_send()
                wait_for(k.send_t.at[level, r], k.ts.at[level, r])

    for level in range(levels):
        final = level + 1 == levels
        if final:
            if level == 0:
                start_pool()
            with scope("backward_enter"):
                backward_enter()
        with scope(f"scalars{level}"):
            take_scalars(level)
            if not final:
                send_scalars(level + 1)
        for h in range(heads):
            with scope(f"states{level}_{h}"):
                for r in leading:
                    take_state(level, r, h)
                    if not final:
                        send_state(level + 1, r, h)
            if final:
                with scope(f"finish{h}"):
                    for j in range(2):
                        k.mem_out[h, rows_of(others[j])] = finish(others[j], h)
                        mem_copies[h][j].start()
            elif level == 0 and h == 0:
                with scope("pooling"):
                    start_pool()
    with scope("finish_near"):
        for h in range(heads):
            k.mem_out[h, rows_of(near)] = finish(near, h)
            mem_copies[h][2].start()
    with scope("finish_own"):
        for h in range(heads):
            k.lhs_mem[h, :, own_cols] = finish(group, h)
    with scope("pool_product"):
        pool_product()

    tile = 512
    for h in range(heads):
        with scope(f"wait_mem{h}"):
            wait_for(k.mem_out.at[h, pl.ds(0, len(others) * size)], k.mr.at[h])
            if h == 0:
                wait_for(k.wmo, k.load_sem.at[3])
        with scope(f"product{h}"):
            for n in range(model_width // tile):
                cols = slice(n * tile, (n + 1) * tile)
                total = k.acc[:, cols] + jnp.dot(
                    k.lhs_mem[h], k.wmo[h, :, cols], preferred_element_type=F32
                )
                if h + 1 < heads:
                    k.acc[:, cols] = total
                else:
                    k.out[:, cols] = total.astype(BF16)

    with scope("leave"):
        wait_for(k.held, k.tp_send)
        wait_for(k.pool_out.at[pl.ds(0, len(others) * size)], k.pool_send)
        wait_for(k.mem_out.at[:, pl.ds(0, len(others) * size)], k.mem_send)
        for level in range(levels):
            settle(level)
        for side in range(2):
            @pl.when(rim_sends[side])
            def _():
                rim(side).wait_send()


def per_device(
    tokens,
    input_norm_gain,
    pooling_input_matrix,
    query_projection_matrix,
    key_projection_matrix,
    value_projection_matrix,
    output_gate_matrix,
    input_gate_matrix,
    forget_gate_matrix,
    forget_gate_bias,
    log_forget_scale,
    extra_log_forget,
    starting_memory,
    starting_normalizer,
    starting_log_scale,
    pooling_group_map,
    pooling_channel_scale,
    memory_head_gain,
    pooling_output_matrix,
    memory_output_matrix,
):
    rows, own_width = tokens.shape
    tp_size = lax.axis_size("tp")
    sp_size = lax.axis_size("sp")
    model_width = own_width * tp_size
    group_dim = pooling_input_matrix.shape[1]
    heads = query_projection_matrix.shape[1] // DH
    mem_width = heads * DH
    pairs = 2 * heads
    levels = max(1, (sp_size - 1).bit_length())
    blocks = tp_size
    size = rows // blocks
    pool_total = pooling_output_matrix.shape[0]
    mem_total = memory_output_matrix.shape[0]
    hbm = pl.BlockSpec(memory_space=pltpu.HBM)
    dma = pltpu.SemaphoreType.DMA
    small = dict(
        gin=input_gate_matrix.transpose(1, 2, 0),
        gfg=forget_gate_matrix.transpose(1, 2, 0),
        gain=input_norm_gain.reshape(1, model_width),
        scale=log_forget_scale,
        extra=extra_log_forget,
        bias=forget_gate_bias,
        start_mem=starting_memory,
        start_norm=starting_normalizer,
        start_log=starting_log_scale,
        map=pooling_group_map,
        pscale=pooling_channel_scale.reshape(1, pool_total),
        hgain=memory_head_gain.reshape(1, mem_total),
    )
    inputs = dict(
        tokens=tokens,
        **{name + "_in": small[name] for name in SMALL},
        wp_hbm=pooling_input_matrix,
        wq_hbm=query_projection_matrix,
        wk_hbm=key_projection_matrix,
        wv_hbm=value_projection_matrix,
        wo_hbm=output_gate_matrix,
        wpo_hbm=pooling_output_matrix,
        wmo_hbm=memory_output_matrix,
    )
    scratch = dict(
        **{name: VMEM(small[name].shape, small[name].dtype) for name in SMALL},
        own=VMEM((rows, own_width), BF16),
        held=VMEM((3, rows, own_width), BF16),
        normed=VMEM((size, model_width), BF16),
        wpg=VMEM((model_width, group_dim + 128), BF16),
        weights=VMEM((4, model_width, mem_width), BF16),
        wpo=VMEM((pool_total, model_width), BF16),
        wmo=VMEM((heads, tp_size * DH, model_width), BF16),
        lhs_mem=VMEM((heads, size, tp_size * DH), BF16),
        acc=VMEM((size, model_width), F32),
        sums=VMEM((size, 2 * size), BF16),
        ext=VMEM((rows + 2 * RIM, group_dim), F32),
        q=VMEM((rows, mem_width), BF16),
        k=VMEM((rows, mem_width), BF16),
        v=VMEM((rows, mem_width), BF16),
        o=VMEM((rows, mem_width), BF16),
        gates=VMEM((2 * pairs, size), F32),
        lifted=VMEM((pairs, size), F32),
        vt=VMEM((heads, AUG, size), BF16),
        adds=VMEM((heads, blocks, AUG, DH), F32),
        ends=VMEM((blocks, 2 * pairs, 128), F32),
        fcum=VMEM((blocks, pairs, 128), F32),
        peaks=VMEM((blocks, pairs, size), F32),
        locals=VMEM((pairs, blocks, AUG, size), F32),
        gated=VMEM((heads, blocks, DH, size), F32),
        cur_t=VMEM((pairs, AUG, DH), F32),
        cur_s=VMEM((2 * pairs, 128), F32),
        enter_t=VMEM((1, heads, AUG, DH), BF16),
        enter_s=VMEM((1, heads, 128), F32),
        back_t=VMEM((heads, blocks, AUG, DH), BF16),
        back_f=VMEM((heads, AUG, DH), F32),
        back_s=VMEM((blocks, heads, 128), F32),
        inc_s=VMEM((2, 2 * heads, 128), F32),
        exc_t=VMEM((pairs, AUG, DH), F32),
        exc_s=VMEM((2, 2 * heads, 128), F32),
        weigh=VMEM((2, 4 * heads, 128), F32),
        send_t=VMEM((levels, 2, heads, AUG, DH), BF16),
        send_s=VMEM((levels, 2, 2 * heads, 128), F32),
        recv_t=VMEM((levels, 2, heads, AUG, DH), BF16),
        recv_s=VMEM((levels, 2, 2 * heads, 128), F32),
        rim_out=VMEM((2, RIM, group_dim), BF16),
        rims=VMEM((2, RIM, group_dim), BF16),
        pool_out=VMEM((rows, group_dim), BF16),
        mem_out=VMEM((heads, rows, DH), BF16),
        lhs_pool=VMEM((size, pool_total), BF16),
        token_sem=dma((2,)),
        small_sem=dma((len(SMALL),)),
        load_sem=dma((4,)),
        tp_send=dma,
        pool_send=dma,
        mem_send=dma,
        near_recv=dma,
        far_recv=dma((blocks + 1,)),
        pass_recv=dma((blocks + 1,)),
        ts=dma((levels, 2)),
        tr=dma((levels, 2, heads)),
        ss=dma((levels, 2)),
        sr=dma((levels, 2)),
        rs=dma((2,)),
        rr=dma((2,)),
        pr=dma,
        mr=dma((heads,)),
    )
    names = tuple(inputs) + ("out",) + tuple(scratch)
    return pl.pallas_call(
        functools.partial(layer_kernel, tp_size, sp_size, heads, names),
        out_shape=VMEM((size, model_width), BF16),
        in_specs=[hbm] * len(inputs),
        out_specs=pl.BlockSpec(memory_space=pltpu.VMEM),
        scratch_shapes=list(scratch.values()),
        compiler_params=pltpu.CompilerParams(
            collective_id=0, has_side_effects=True, vmem_limit_bytes=KERNEL_VMEM
        ),
    )(*(pltpu.with_memory_space_constraint(value, pltpu.HBM) for value in inputs.values()))


def solution(mesh):
    placed = (
        P("sp", "tp"),
        P(),
        P(None, "tp"),
        P(None, "tp"),
        P(None, "tp"),
        P(None, "tp"),
        P(None, "tp"),
        P(),
        P(),
        P(),
        P(None, "sp"),
        P(None, "sp"),
        P(None, "tp", None, None),
        P(None, "tp", None),
        P(None, "tp"),
        P(),
        P(),
        P(),
        P(),
        P(),
    )
    return jax.shard_map(
        per_device, mesh=mesh, in_specs=placed, out_specs=P(("sp", "tp"), None), check_vma=False
    )
```

```python
import contextlib
import functools
import types

import jax
import jax.numpy as jnp
from jax import lax
from jax.experimental import pallas as pl
from jax.experimental.pallas import tpu as pltpu
from jax.sharding import PartitionSpec as P

DH = 128
NEG_BIG = -1e30
LN_EPS = 1e-05
HEAD_EPS = 1e-06
RIM = 16
AUG = 144
VMEM = pltpu.VMEM
MESH = pl.DeviceIdType.MESH
F32 = jnp.float32
BF16 = jnp.bfloat16
PROFILE = False
KERNEL_VMEM = 48 * 1024 * 1024
SMALL = (
    "gin", "gfg", "gain", "scale", "extra", "bias", "start_mem", "start_norm", "start_log",
    "map", "pscale", "hgain",
)


def scope(name):
    return jax.named_scope(name) if PROFILE else contextlib.nullcontext()


def scan_lanes(values, combine, neutral, forward_rows):
    lanes = values.shape[1]
    lane = lax.broadcasted_iota(jnp.int32, values.shape, 1)
    forward = lax.broadcasted_iota(jnp.int32, values.shape, 0) < forward_rows
    shift = 1
    while shift < lanes:
        low = jnp.where(lane >= shift, pltpu.roll(values, shift, 1), neutral)
        high = jnp.where(lane < lanes - shift, pltpu.roll(values, lanes - shift, 1), neutral)
        values = combine(values, jnp.where(forward, low, high))
        shift *= 2
    return values


def split_three(values):
    high = values.astype(BF16)
    rest = values - high.astype(F32)
    middle = rest.astype(BF16)
    low = (rest - middle.astype(F32)).astype(BF16)
    return high.astype(F32), middle.astype(F32), low.astype(F32)


def wide(row, lanes):
    return jnp.concatenate([row] * (lanes // row.shape[1]), axis=1)


def layer_kernel(tp_size, sp_size, heads, names, *refs):
    k = types.SimpleNamespace(**dict(zip(names, refs, strict=True)))
    me = lax.axis_index("sp")
    group = lax.axis_index("tp")
    far = lax.rem(group + tp_size // 2, tp_size)
    near = group + 1 - 2 * lax.rem(group, 2)
    diagonal = lax.rem(near + tp_size // 2, tp_size)
    others = (far, diagonal, near)
    rows_total, width = k.tokens.shape
    small_refs = [(getattr(k, name + "_in"), getattr(k, name)) for name in SMALL]
    model_width = width * tp_size
    blocks = tp_size
    size = rows_total // blocks
    half = size // 2
    pairs = 2 * heads
    all_heads = k.gin.shape[1]
    group_dim = k.map.shape[1]
    mem_width = heads * DH
    last = blocks - 1
    odd = lax.rem(me, 2)
    partner = me + 1 - 2 * odd
    strides = [1]
    while strides[-1] * 2 < sp_size:
        strides.append(strides[-1] * 2)
    levels = len(strides)

    def route(level, r):
        stride = strides[level]
        if level == 0:
            return True, partner, True
        step = stride * (1 - 2 * r)
        target, source = me + step, me - step
        okay = jnp.logical_and(target >= 0, target < sp_size)
        has = jnp.logical_and(source >= 0, source < sp_size)
        return okay, target, has

    late_half = (me >= sp_size // 2).astype(jnp.int32)
    leading = (late_half, 1 - late_half)

    def when(condition):
        if condition is True:
            return lambda body: body()
        return pl.when(condition)

    rim_sends = (me + 1 < sp_size, me >= 1)
    rim_recvs = (me >= 1, me + 1 < sp_size)

    barrier = pltpu.get_barrier_semaphore()
    peers = jnp.int32(len(others))
    for other in others:
        pl.semaphore_signal(barrier, inc=1, device_id={"tp": other}, device_id_type=MESH)
    greets = []
    for stride in strides:
        greets += [(me + stride < sp_size, me + stride), (me >= stride, me - stride)]
    for okay, other in greets:
        peers = peers + okay.astype(jnp.int32)

        @pl.when(okay)
        def _():
            pl.semaphore_signal(barrier, inc=1, device_id={"sp": other}, device_id_type=MESH)

    spans = [(b * size, size) for b in range(last)]
    spans += [(last * size, half), (last * size + half, half)]
    token_loads = [
        pltpu.make_async_copy(k.tokens.at[pl.ds(a, n)], k.own.at[pl.ds(a, n)], k.token_sem.at[i])
        for i, (a, n) in enumerate(((0, size), (size, rows_total - size)))
    ]
    for load in token_loads:
        load.start()

    def load_all(pairs_of, semaphore):
        for source, target in pairs_of:
            pltpu.make_async_copy(source, target, semaphore).start()

    def wait_for(ref, semaphore):
        pltpu.make_async_copy(ref, ref, semaphore).wait()

    def own_rows(ref, r):
        mine = ref[r, 0:heads, :].astype(F32)
        for other in range(1, tp_size):
            mine = jnp.where(
                group == other, ref[r, other * heads : (other + 1) * heads, :].astype(F32), mine
            )
        return mine

    with scope("barrier"):
        pl.semaphore_wait(barrier, peers)

    def to_tp(source, target, send, recv, other):
        return pltpu.make_async_remote_copy(
            src_ref=source, dst_ref=target, send_sem=send, recv_sem=recv,
            device_id={"tp": other}, device_id_type=MESH,
        )

    def to_sp(source, target, send, recv, other):
        return pltpu.make_async_remote_copy(
            src_ref=source, dst_ref=target, send_sem=send, recv_sem=recv,
            device_id={"sp": other}, device_id_type=MESH,
        )

    to_far, onward = [], []
    to_near = to_tp(k.own, k.held.at[0], k.tp_send, k.near_recv, near)
    for i, (a, n) in enumerate(spans):
        s = pl.ds(a, n)
        to_far.append(to_tp(k.own.at[s], k.held.at[1, s], k.tp_send, k.far_recv.at[i], far))
        onward.append(
            to_tp(k.held.at[1, s], k.held.at[2, s], k.tp_send, k.pass_recv.at[i], near)
        )
    token_loads[0].wait()
    to_far[0].start()
    token_loads[1].wait()
    for copy in to_far[1:]:
        copy.start()
    to_near.start()
    smalls = [
        pltpu.make_async_copy(source, target, k.small_sem.at[i])
        for i, (source, target) in enumerate(small_refs)
    ]
    for load in smalls:
        load.start()
    pool_weight = pltpu.make_async_copy(
        k.wp_hbm, k.wpg.at[:, pl.ds(0, group_dim)], k.load_sem.at[0]
    )
    pool_weight.start()
    wk, wv, wq, wo = (k.weights.at[i] for i in range(4))
    load_all(
        ((k.wk_hbm, wk), (k.wv_hbm, wv), (k.wq_hbm, wq), (k.wo_hbm, wo)), k.load_sem.at[1]
    )

    mem_rows = [
        (k.wmo_hbm.at[pl.ds((g * heads + h) * DH, DH)], k.wmo.at[h, pl.ds(g * DH, DH)])
        for h in range(heads)
        for g in range(tp_size)
    ]
    out_weight = pltpu.make_async_copy(k.wpo_hbm, k.wpo, k.load_sem.at[2])
    out_weight.start()
    load_all(mem_rows, k.load_sem.at[3])
    for load in smalls:
        load.wait()

    bias_lane = lax.broadcasted_iota(jnp.int32, k.bias.shape, 1)
    picked = [
        jnp.sum(jnp.where(bias_lane == group * heads + h, k.bias[...], 0.0), axis=1, keepdims=True)
        for h in range(heads)
    ]
    bias = jnp.concatenate([picked[h][r : r + 1] for r in range(2) for h in range(heads)], axis=0)

    s_at = lax.broadcasted_iota(jnp.int32, (size, size), 0)
    t_at = lax.broadcasted_iota(jnp.int32, (size, size), 1)

    def gate_weights():
        gate_rows = jnp.concatenate([own_rows(ref, r) for ref in (k.gin, k.gfg) for r in range(2)], axis=0)
        gate_rows = jnp.concatenate(
            [gate_rows, jnp.zeros((128 - 2 * pairs, model_width), F32)], axis=0
        )
        for n in range(model_width // 128):
            at = slice(n * 128, (n + 1) * 128)
            k.wpg[at, group_dim : group_dim + 128] = jnp.transpose(gate_rows[:, at]).astype(BF16)
        k.sums[:, 0:size] = (s_at <= t_at).astype(F32).astype(BF16)
        k.sums[:, size : 2 * size] = (s_at >= t_at).astype(F32).astype(BF16)

    def both_rows(ref, span):
        return jnp.concatenate(
            [jnp.broadcast_to(ref[r : r + 1, span], (heads, size)) for r in range(2)], axis=0
        )

    def add_sums(sums, view):
        part = view.astype(F32)
        return (
            sums[0] + jnp.sum(part, axis=1, keepdims=True),
            sums[1] + jnp.sum(part * part, axis=1, keepdims=True),
        )

    def early_sums(a, n):
        rows = slice(a, a + n)
        sums = (jnp.zeros((n, 1), F32), jnp.zeros((n, 1), F32))
        for view in (k.own[rows, :], k.held[0, rows, :], k.held[1, rows, :]):
            sums = add_sums(sums, view)
        return sums

    def normalize(a, n, at, sums):
        rows = slice(a, a + n)
        views = [k.own[rows, :]] + [k.held[slot, rows, :] for slot in range(3)]
        total, square = add_sums(sums, views[3])
        mean = total / model_width
        inverse = lax.rsqrt(square / model_width - mean * mean + LN_EPS)
        for view, owner in zip(views, (group, near, far, diagonal)):
            columns = pl.ds(pl.multiple_of(owner * width, width), width)
            k.normed[at : at + n, columns] = (
                (view.astype(F32) - mean) * inverse * k.gain[:, columns]
            ).astype(BF16)

    def project(a, n, at, targets):
        x = k.normed[at : at + n, :]
        for weight, target in targets:
            target[a : a + n, :] = jnp.dot(x, weight[...], preferred_element_type=F32).astype(BF16)

    def project_gates(a, n, at):
        x = k.normed[at : at + n, :]
        mixed = jnp.dot(x, k.wpg[...], preferred_element_type=F32)
        k.ext[RIM + a : RIM + a + n, :] = mixed[:, :group_dim].astype(BF16).astype(F32)
        k.gates[:, at : at + n] = jnp.transpose(mixed[:, group_dim:])[: 2 * pairs]

    zero_state = jnp.zeros((AUG, DH), F32)

    def initial(r, h):
        is_first = me == (0 if r == 0 else sp_size - 1)
        begin = jnp.broadcast_to(k.start_log[r : r + 1, h : h + 1], (1, 128))
        level = jnp.where(is_first, begin, NEG_BIG)
        rows = jnp.concatenate(
            [k.start_mem[r, h], jnp.broadcast_to(k.start_norm[r, h : h + 1, :], (AUG - DH, DH))], axis=0
        )
        return jnp.where(is_first, rows, 0.0), level

    def prepare():
        for h in range(heads):
            state, level = initial(0, h)
            k.cur_t[h] = state
            k.cur_s[h : h + 1, :] = level
            k.cur_t[heads + h] = zero_state
            k.cur_s[heads + h : heads + h + 1, :] = jnp.full((1, 128), NEG_BIG, F32)
        k.cur_s[pairs : 2 * pairs, :] = jnp.zeros((pairs, 128), F32)

    def summary(b):
        span = slice(b * size, (b + 1) * size)
        pre = k.gates[pairs : 2 * pairs, :] + bias
        log_sig = jnp.minimum(pre, 0.0) - jnp.log1p(jnp.exp(-jnp.abs(pre)))
        log_fg = log_sig * both_rows(k.scale, span) + both_rows(k.extra, span)
        parts = jnp.concatenate(split_three(log_fg), axis=0).astype(BF16)
        sums = jnp.dot(parts, k.sums[...], preferred_element_type=F32)
        sums = sums[:pairs] + sums[pairs : 2 * pairs] + sums[2 * pairs :]
        falls = jnp.concatenate([sums[:heads, :size], sums[heads:, size:]], axis=0)
        lifted = k.gates[:pairs, :] - falls
        top = jnp.max(lifted, axis=1, keepdims=True)
        sources = lifted + jnp.log(F32(DH ** -0.5))
        k.lifted[...] = lifted
        weights = jnp.exp(sources - top)
        peaks = jnp.broadcast_to(top, (pairs, 128))
        fall = jnp.concatenate(
            [falls[:heads, size - 1 : size], falls[heads:, 0:1]], axis=0
        )
        fall = jnp.broadcast_to(fall, (pairs, 128))
        for h in range(heads):
            cols = slice(h * DH, (h + 1) * DH)
            keys = k.k[span, cols]
            vt = jnp.concatenate(
                [jnp.transpose(k.v[span, cols].astype(F32)), jnp.ones((AUG - DH, size), F32)], axis=0
            )
            k.vt[h] = vt.astype(BF16)
            adds = [
                jnp.dot(
                    (vt * weights[p : p + 1]).astype(BF16), keys, preferred_element_type=F32
                )
                for p in (h, heads + h)
            ]
            p = h
            peak, down = peaks[p : p + 1], fall[p : p + 1]
            level = k.cur_s[p : p + 1, :]
            k.enter_t[0, h] = k.cur_t[p].astype(BF16)
            k.enter_s[0, h : h + 1, :] = level
            k.fcum[b, p : p + 1, :] = k.cur_s[pairs + p : pairs + p + 1, :]
            joint = jnp.maximum(level, peak)
            k.cur_t[p] = jnp.exp(level - joint) * k.cur_t[p] + jnp.exp(peak - joint) * adds[0]
            k.cur_s[p : p + 1, :] = joint + down
            k.cur_s[pairs + p : pairs + p + 1, :] += down
            p = heads + h
            peak, down = peaks[p : p + 1], fall[p : p + 1]
            k.ends[b, p : p + 1, :] = peak
            k.ends[b, pairs + p : pairs + p + 1, :] = down
            late = k.cur_s[p : p + 1, :]
            late_fall = k.cur_s[pairs + p : pairs + p + 1, :]
            if b < last:
                k.adds[h, b] = adds[1]
                early, level = adds[1], peak + down
            else:
                state, level = initial(1, h)
                k.back_t[h, b] = state.astype(BF16)
                k.back_s[b, h : h + 1, :] = level
                joint = jnp.maximum(level, peak)
                early = jnp.exp(level - joint) * state + jnp.exp(peak - joint) * adds[1]
                level = joint + down
                if b > 0:
                    k.back_f[h] = early
                    k.back_s[b - 1, h : h + 1, :] = level
            level = level + late_fall
            joint = jnp.maximum(level, late)
            k.cur_t[p] = jnp.exp(level - joint) * early + jnp.exp(late - joint) * k.cur_t[p]
            k.cur_s[p : p + 1, :] = joint
            k.cur_s[pairs + p : pairs + p + 1, :] = late_fall + down

    def local_block(b):
        span = slice(b * size, (b + 1) * size)
        lifted = k.lifted[...]
        peaks = scan_lanes(lifted, jnp.maximum, NEG_BIG, heads)
        levels_in = jnp.concatenate(
            [wide(k.enter_s[0, 0:heads, :], size), jnp.full((heads, size), NEG_BIG, F32)], axis=0
        )
        peaks = jnp.maximum(peaks, levels_in)
        k.peaks[b, 0:pairs, :] = peaks
        carry = jnp.exp(levels_in[:heads] - peaks[:heads])
        sources = lifted + jnp.log(F32(DH ** -0.5))
        columns = jnp.transpose(
            jnp.concatenate([sources, jnp.zeros((128 - pairs, size), F32)], axis=0)
        )
        for h in range(heads):
            cols = slice(h * DH, (h + 1) * DH)
            queries = k.q[span, cols]
            scores = lax.dot_general(
                k.k[span, cols], queries, (((1,), (1,)), ((), ())), preferred_element_type=F32
            )
            values = k.vt[h]
            before = lax.dot_general(
                k.enter_t[0, h], queries, (((1,), (1,)), ((), ())), preferred_element_type=F32
            )
            for r in range(2):
                p = r * heads + h
                inside = (s_at <= t_at) if r == 0 else (s_at >= t_at)
                weight = jnp.exp(
                    jnp.where(inside, columns[:, p : p + 1] - peaks[p : p + 1], NEG_BIG)
                )
                result = jnp.dot(
                    values, (scores * weight).astype(BF16), preferred_element_type=F32
                )
                if r == 0:
                    result = result + carry[h : h + 1] * before
                k.locals[p, b] = result

    def out_gates(b):
        span = slice(b * size, (b + 1) * size)
        for h in range(heads):
            opened = jnp.transpose(k.o[span, h * DH : (h + 1) * DH].astype(F32))
            gain = k.hgain[:, pl.ds(pl.multiple_of(group * mem_width + h * DH, DH), DH)]
            column = jnp.transpose(jnp.broadcast_to(gain, (128, DH)))
            k.gated[h, b] = wide(column, size) / (1.0 + jnp.exp(-opened))

    with scope("prepare"):
        gate_weights()
        prepare()
    def rim(side):
        other = me + 1 if side == 0 else me - 1
        return to_sp(k.rim_out.at[side], k.rims.at[side], k.rs.at[side], k.rr.at[side], other)

    def start_rims():
        k.rim_out[1] = k.ext[RIM : 2 * RIM, :].astype(BF16)
        k.rim_out[0] = k.ext[rows_total : RIM + rows_total, :].astype(BF16)
        for side in range(2):
            @pl.when(rim_sends[side])
            def _():
                rim(side).start()

    def pass_on(i):
        to_far[i].wait_recv()
        onward[i].start()

    for b in range(blocks):
        pieces = [i for i, (a, n) in enumerate(spans) if b * size <= a < (b + 1) * size]
        with scope(f"far{b}"):
            for i in pieces[1 if b == last and b > 0 else 0 :]:
                pass_on(i)
        for i in pieces:
            a, n = spans[i]
            at = a - b * size
            if i == 0:
                to_near.wait_recv()
            with scope(f"wait{i}"):
                sums = early_sums(a, n)
                onward[i].wait_recv()
            if i == 0:
                pool_weight.wait()
                wait_for(k.weights, k.load_sem.at[1])
            with scope(f"project{i}"):
                normalize(a, n, at, sums)
                project_gates(a, n, at)
                project(a, n, at, ((wk, k.k), (wv, k.v)))
        if b == last - 1:
            with scope("far_half"):
                pass_on(last)
        if b < last:
            with scope(f"local{b}"):
                project(b * size, size, 0, ((wq, k.q), (wo, k.o)))
                summary(b)
                local_block(b)
                out_gates(b)
        else:
            with scope(f"summary{b}"):
                start_rims()
                summary(b)

    for r in range(2):
        for h in range(heads):
            p = r * heads + h
            k.inc_s[r, h : h + 1, :] = k.cur_s[p : p + 1, :]
            k.inc_s[r, heads + h : heads + h + 1, :] = k.cur_s[pairs + p : pairs + p + 1, :]

    def scalar_copy(level, r):
        return to_sp(
            k.send_s.at[level, r], k.recv_s.at[level, r], k.ss.at[level, r], k.sr.at[level, r],
            route(level, r)[1],
        )

    def state_copy(level, r, h):
        return to_sp(
            k.send_t.at[level, r, h], k.recv_t.at[level, r, h], k.ts.at[level, r],
            k.tr.at[level, r, h], route(level, r)[1],
        )

    def ready(slot, level, r):
        okay = route(level, r)[0]
        if slot >= 2:
            okay = jnp.logical_and(okay, route(slot - 1, r)[2])
        if level > slot:
            okay = jnp.logical_and(okay, jnp.logical_not(route(slot, r)[2]))
        return okay

    def send_scalars(slot):
        for r in range(2):
            for level in range(slot, levels if slot > 0 else 1):
                @when(ready(slot, level, r))
                def _():
                    k.send_s[level, r] = k.inc_s[r]
                    scalar_copy(level, r).start()

    def send_state(slot, r, h):
        for level in range(slot, levels if slot > 0 else 1):
            @when(ready(slot, level, r))
            def _():
                k.send_t[level, r, h] = k.cur_t[r * heads + h].astype(BF16)
                state_copy(level, r, h).start()

    def take_scalars(level):
        for r in range(2):
            @when(route(level, r)[2])
            def _():
                scalar_copy(level, r).wait_recv()
                theirs_max = k.recv_s[level, r, 0:heads, :]
                theirs_fall = k.recv_s[level, r, heads : 2 * heads, :]
                own_max = k.inc_s[r, 0:heads, :]
                own_fall = k.inc_s[r, heads : 2 * heads, :]
                if level == 0:
                    early = (odd == 1) if r == 0 else (odd == 0)
                    a = jnp.where(early, theirs_max + own_fall, theirs_max)
                    c = jnp.where(early, own_max, own_max + theirs_fall)
                    flag = jnp.where(early, 1.0, 0.0).astype(F32)
                    k.weigh[r, 2 * heads : 3 * heads, :] = jnp.full((heads, 128), flag, F32)
                    k.exc_s[r, 0:heads, :] = jnp.where(early, theirs_max, NEG_BIG)
                    k.exc_s[r, heads : 2 * heads, :] = jnp.where(early, theirs_fall, 0.0)
                else:
                    a = theirs_max + own_fall
                    c = own_max
                    late_max = k.exc_s[r, 0:heads, :]
                    late_fall = k.exc_s[r, heads : 2 * heads, :]
                    level_in = theirs_max + late_fall
                    top = jnp.maximum(level_in, late_max)
                    k.weigh[r, 2 * heads : 3 * heads, :] = jnp.exp(level_in - top)
                    k.weigh[r, 3 * heads : 4 * heads, :] = jnp.exp(late_max - top)
                    k.exc_s[r, 0:heads, :] = top
                    k.exc_s[r, heads : 2 * heads, :] = theirs_fall + late_fall
                top = jnp.maximum(a, c)
                k.weigh[r, 0:heads, :] = jnp.exp(a - top)
                k.weigh[r, heads : 2 * heads, :] = jnp.exp(c - top)
                k.inc_s[r, 0:heads, :] = top
                k.inc_s[r, heads : 2 * heads, :] = theirs_fall + own_fall

    def take_state(level, r, h):
        @when(route(level, r)[2])
        def _():
            state_copy(level, r, h).wait_recv()
            p = r * heads + h
            arrived = k.recv_t[level, r, h].astype(F32)
            if level + 1 < levels:
                k.cur_t[p] = (
                    k.weigh[r, h : h + 1, :] * arrived
                    + k.weigh[r, heads + h : heads + h + 1, :] * k.cur_t[p]
                )
            mine = k.weigh[r, 2 * heads + h : 2 * heads + h + 1, :] * arrived
            if level > 0:
                mine = mine + k.weigh[r, 3 * heads + h : 3 * heads + h + 1, :] * k.exc_t[p]
            k.exc_t[p] = mine

    def pooling():
        for side in range(2):
            at = 0 if side == 0 else RIM + rows_total

            @pl.when(rim_recvs[side])
            def _():
                rim(side).wait_recv()
                k.ext[at : at + RIM, :] = k.rims[side].astype(F32)

            @pl.when(jnp.logical_not(rim_recvs[side]))
            def _():
                k.ext[at : at + RIM, :] = jnp.zeros((RIM, group_dim), F32)
        half_span = jnp.left_shift(jnp.int32(1), group)
        for n in range(blocks):
            first = n * size
            chunk = k.ext[first : first + size + 2 * RIM, :]
            own = chunk[RIM : RIM + size]
            low = 1
            running = chunk[: size + 2 * RIM - 1] + chunk[1:]
            reach = 1
            while 2 * reach < RIM:
                span = running.shape[0] - 2 * reach
                longer = running[:span] + running[2 * reach :]
                kept = running[reach : reach + span]
                running = jnp.where(half_span > reach, longer, kept)
                low += reach
                reach *= 2
            pooled = running[RIM - low : RIM - low + size]
            position = me * rows_total + first + lax.broadcasted_iota(jnp.int32, own.shape, 0)
            count = jnp.minimum(position + half_span, rows_total * sp_size) - jnp.maximum(
                position - half_span, 0
            )
            contrast = (pooled / count.astype(F32) - own).astype(BF16)
            mapped = jnp.dot(contrast, k.map[group], preferred_element_type=F32)
            scale = k.pscale[:, pl.ds(pl.multiple_of(group * group_dim, group_dim), group_dim)]
            k.pool_out[first : first + size, :] = (mapped * scale).astype(BF16)

    pool_cols = pl.ds(pl.multiple_of(group * group_dim, group_dim), group_dim)

    def rows_of(owner):
        return pl.ds(pl.multiple_of(owner * size, size), size)

    own_cols = pl.ds(pl.multiple_of(group * DH, DH), DH)

    pool_copies = [
        to_tp(k.pool_out.at[rows_of(other)], k.lhs_pool.at[:, pool_cols], k.pool_send, k.pr, other)
        for j, other in enumerate(others)
    ]
    mem_copies = [
        [
            to_tp(
                k.mem_out.at[h, rows_of(other)], k.lhs_mem.at[h, :, own_cols],
                k.mem_send, k.mr.at[h] if j < 2 else k.mn.at[h], other,
            )
            for j, other in enumerate(others)
        ]
        for h in range(heads)
    ]

    def start_pool():
        pooling()
        for copy in pool_copies:
            copy.start()

    home = pl.ds(pl.multiple_of(lax.div(group, 2) * 2 * DH, 2 * DH), 2 * DH)
    away = pl.ds(pl.multiple_of(lax.div(far, 2) * 2 * DH, 2 * DH), 2 * DH)
    tile = 512

    def mem_product(h, span, cols):
        return jnp.dot(k.lhs_mem[h, :, span], k.wmo[h, span, cols], preferred_element_type=F32)

    def home_product():
        k.lhs_pool[:, pool_cols] = k.pool_out[rows_of(group), :]
        wait_for(k.pool_out.at[pl.ds(0, len(others) * size)], k.pr)
        out_weight.wait()
        wait_for(k.wmo, k.load_sem.at[3])
        for h in range(heads):
            wait_for(k.mem_out.at[h, pl.ds(0, size)], k.mn.at[h])
        for n in range(model_width // tile):
            cols = slice(n * tile, (n + 1) * tile)
            total = jnp.dot(k.lhs_pool[...], k.wpo[:, cols], preferred_element_type=F32)
            for h in range(heads):
                total = total + mem_product(h, home, cols)
            k.acc[:, cols] = total

    def last_local():
        project(last * size, size, 0, ((wq, k.q), (wo, k.o)))
        local_block(last)
        out_gates(last)

    def backward_enter():
        for h in range(heads):
            p = heads + h
            fall = k.ends[last, pairs + p : pairs + p + 1, :]
            k.fcum[last, p : p + 1, :] = jnp.zeros((1, 128), F32)
            if blocks > 1:
                state, level = k.back_f[h], k.back_s[last - 1, h : h + 1, :]
            for b in reversed(range(last)):
                k.back_t[h, b] = state.astype(BF16)
                k.fcum[b, p : p + 1, :] = fall
                if b > 0:
                    peak = k.ends[b, p : p + 1, :]
                    down = k.ends[b, pairs + p : pairs + p + 1, :]
                    joint = jnp.maximum(level, peak)
                    state = jnp.exp(level - joint) * state + jnp.exp(peak - joint) * k.adds[h, b]
                    level = joint + down
                    k.back_s[b - 1, h : h + 1, :] = level
                    fall = fall + down
        for b in range(blocks):
            span = slice(b * size, (b + 1) * size)
            for h in range(heads):
                p = heads + h
                level = wide(k.back_s[b, h : h + 1, :], size)
                peak = k.peaks[b, p : p + 1, :]
                joint = jnp.maximum(level, peak)
                before = lax.dot_general(
                    k.back_t[h, b], k.q[span, h * DH : (h + 1) * DH], (((1,), (1,)), ((), ())),
                    preferred_element_type=F32,
                )
                k.locals[p, b] = (
                    jnp.exp(peak - joint) * k.locals[p, b] + jnp.exp(level - joint) * before
                )
                k.peaks[b, p : p + 1, :] = joint

    def finish(b, h):
        states = jnp.concatenate([k.exc_t[h], k.exc_t[heads + h]], axis=0).astype(BF16)
        queries = k.q[rows_of(b), h * DH : (h + 1) * DH]
        entered = lax.dot_general(
            states, queries, (((1,), (1,)), ((), ())), preferred_element_type=F32
        )
        hidden = None
        for r in range(2):
            p = r * heads + h
            level = wide(k.exc_s[r, h : h + 1, :] + k.fcum[b, p : p + 1, :], size)
            peak = k.peaks[b, p : p + 1, :]
            joint = jnp.maximum(level, peak)
            a = jnp.exp(peak - joint)
            c = jnp.exp(level - joint)
            mine = k.locals[p, b]
            theirs = entered[r * AUG : (r + 1) * AUG]
            below = a * mine[DH : DH + 1] + c * theirs[DH : DH + 1]
            inverse = 1.0 / jnp.maximum(jnp.abs(below), 1.0)
            part = (a * inverse) * mine[:DH] + (c * inverse) * theirs[:DH]
            hidden = part if hidden is None else hidden + part
        centered = hidden - jnp.mean(hidden, axis=0, keepdims=True)
        variance = jnp.mean(centered * centered, axis=0, keepdims=True)
        scaled = centered * lax.rsqrt(variance + HEAD_EPS) * k.gated[h, b]
        return jnp.transpose(scaled).astype(BF16)

    with scope("send0"):
        send_scalars(0)
        for h in range(heads):
            for r in leading:
                send_state(0, r, h)
        wait_for(k.held, k.tp_send)
    for r in range(2):
        for h in range(heads):
            k.exc_t[r * heads + h] = zero_state
    with scope("last_local"):
        last_local()

    def settle(level):
        for r in range(2):
            @when(route(level, r)[0])
            def _():
                scalar_copy(level, r).wait_send()
                wait_for(k.send_t.at[level, r], k.ts.at[level, r])

    for level in range(levels):
        final = level + 1 == levels
        if final:
            if level == 0:
                start_pool()
            with scope("backward_enter"):
                backward_enter()
        with scope(f"scalars{level}"):
            take_scalars(level)
            if not final:
                send_scalars(level + 1)
        for h in range(heads):
            with scope(f"states{level}_{h}"):
                for r in leading:
                    take_state(level, r, h)
                    if not final:
                        send_state(level + 1, r, h)
            if final:
                with scope(f"finish{h}"):
                    for j in range(2):
                        k.mem_out[h, rows_of(others[j])] = finish(others[j], h)
                        mem_copies[h][j].start()
                if h == 0:
                    settle(0)
                with scope(f"finish_near{h}"):
                    k.mem_out[h, rows_of(near)] = finish(near, h)
                    mem_copies[h][2].start()
                with scope(f"finish_own{h}"):
                    k.lhs_mem[h, :, own_cols] = finish(group, h)
            elif level == 0 and h == 0:
                with scope("pooling"):
                    start_pool()
    with scope("home_product"):
        home_product()
    for h in range(heads):
        with scope(f"wait_mem{h}"):
            wait_for(k.mem_out.at[h, pl.ds(0, 2 * size)], k.mr.at[h])
        with scope(f"product{h}"):
            for n in range(model_width // tile):
                cols = slice(n * tile, (n + 1) * tile)
                total = k.acc[:, cols] + mem_product(h, away, cols)
                if h + 1 < heads:
                    k.acc[:, cols] = total
                else:
                    k.out[:, cols] = total.astype(BF16)

    with scope("leave"):
        wait_for(k.pool_out.at[pl.ds(0, len(others) * size)], k.pool_send)
        wait_for(k.mem_out.at[:, pl.ds(0, len(others) * size)], k.mem_send)
        for level in range(1, levels):
            settle(level)
        for side in range(2):
            @pl.when(rim_sends[side])
            def _():
                rim(side).wait_send()


def per_device(
    tokens,
    input_norm_gain,
    pooling_input_matrix,
    query_projection_matrix,
    key_projection_matrix,
    value_projection_matrix,
    output_gate_matrix,
    input_gate_matrix,
    forget_gate_matrix,
    forget_gate_bias,
    log_forget_scale,
    extra_log_forget,
    starting_memory,
    starting_normalizer,
    starting_log_scale,
    pooling_group_map,
    pooling_channel_scale,
    memory_head_gain,
    pooling_output_matrix,
    memory_output_matrix,
):
    rows, own_width = tokens.shape
    tp_size = lax.axis_size("tp")
    sp_size = lax.axis_size("sp")
    model_width = own_width * tp_size
    group_dim = pooling_input_matrix.shape[1]
    heads = query_projection_matrix.shape[1] // DH
    mem_width = heads * DH
    pairs = 2 * heads
    levels = max(1, (sp_size - 1).bit_length())
    blocks = tp_size
    size = rows // blocks
    pool_total = pooling_output_matrix.shape[0]
    mem_total = memory_output_matrix.shape[0]
    hbm = pl.BlockSpec(memory_space=pltpu.HBM)
    dma = pltpu.SemaphoreType.DMA
    small = dict(
        gin=input_gate_matrix.transpose(1, 2, 0),
        gfg=forget_gate_matrix.transpose(1, 2, 0),
        gain=input_norm_gain.reshape(1, model_width),
        scale=log_forget_scale,
        extra=extra_log_forget,
        bias=forget_gate_bias,
        start_mem=starting_memory,
        start_norm=starting_normalizer,
        start_log=starting_log_scale,
        map=pooling_group_map,
        pscale=pooling_channel_scale.reshape(1, pool_total),
        hgain=memory_head_gain.reshape(1, mem_total),
    )
    inputs = dict(
        tokens=tokens,
        **{name + "_in": small[name] for name in SMALL},
        wp_hbm=pooling_input_matrix,
        wq_hbm=query_projection_matrix,
        wk_hbm=key_projection_matrix,
        wv_hbm=value_projection_matrix,
        wo_hbm=output_gate_matrix,
        wpo_hbm=pooling_output_matrix,
        wmo_hbm=memory_output_matrix,
    )
    scratch = dict(
        **{name: VMEM(small[name].shape, small[name].dtype) for name in SMALL},
        own=VMEM((rows, own_width), BF16),
        held=VMEM((3, rows, own_width), BF16),
        normed=VMEM((size, model_width), BF16),
        wpg=VMEM((model_width, group_dim + 128), BF16),
        weights=VMEM((4, model_width, mem_width), BF16),
        wpo=VMEM((pool_total, model_width), BF16),
        wmo=VMEM((heads, tp_size * DH, model_width), BF16),
        lhs_mem=VMEM((heads, size, tp_size * DH), BF16),
        acc=VMEM((size, model_width), F32),
        sums=VMEM((size, 2 * size), BF16),
        ext=VMEM((rows + 2 * RIM, group_dim), F32),
        q=VMEM((rows, mem_width), BF16),
        k=VMEM((rows, mem_width), BF16),
        v=VMEM((rows, mem_width), BF16),
        o=VMEM((rows, mem_width), BF16),
        gates=VMEM((2 * pairs, size), F32),
        lifted=VMEM((pairs, size), F32),
        vt=VMEM((heads, AUG, size), BF16),
        adds=VMEM((heads, blocks, AUG, DH), F32),
        ends=VMEM((blocks, 2 * pairs, 128), F32),
        fcum=VMEM((blocks, pairs, 128), F32),
        peaks=VMEM((blocks, pairs, size), F32),
        locals=VMEM((pairs, blocks, AUG, size), F32),
        gated=VMEM((heads, blocks, DH, size), F32),
        cur_t=VMEM((pairs, AUG, DH), F32),
        cur_s=VMEM((2 * pairs, 128), F32),
        enter_t=VMEM((1, heads, AUG, DH), BF16),
        enter_s=VMEM((1, heads, 128), F32),
        back_t=VMEM((heads, blocks, AUG, DH), BF16),
        back_f=VMEM((heads, AUG, DH), F32),
        back_s=VMEM((blocks, heads, 128), F32),
        inc_s=VMEM((2, 2 * heads, 128), F32),
        exc_t=VMEM((pairs, AUG, DH), F32),
        exc_s=VMEM((2, 2 * heads, 128), F32),
        weigh=VMEM((2, 4 * heads, 128), F32),
        send_t=VMEM((levels, 2, heads, AUG, DH), BF16),
        send_s=VMEM((levels, 2, 2 * heads, 128), F32),
        recv_t=VMEM((levels, 2, heads, AUG, DH), BF16),
        recv_s=VMEM((levels, 2, 2 * heads, 128), F32),
        rim_out=VMEM((2, RIM, group_dim), BF16),
        rims=VMEM((2, RIM, group_dim), BF16),
        pool_out=VMEM((rows, group_dim), BF16),
        mem_out=VMEM((heads, rows, DH), BF16),
        lhs_pool=VMEM((size, pool_total), BF16),
        token_sem=dma((2,)),
        small_sem=dma((len(SMALL),)),
        load_sem=dma((4,)),
        tp_send=dma,
        pool_send=dma,
        mem_send=dma,
        near_recv=dma,
        far_recv=dma((blocks + 1,)),
        pass_recv=dma((blocks + 1,)),
        ts=dma((levels, 2)),
        tr=dma((levels, 2, heads)),
        ss=dma((levels, 2)),
        sr=dma((levels, 2)),
        rs=dma((2,)),
        rr=dma((2,)),
        pr=dma,
        mr=dma((heads,)),
        mn=dma((heads,)),
    )
    names = tuple(inputs) + ("out",) + tuple(scratch)
    return pl.pallas_call(
        functools.partial(layer_kernel, tp_size, sp_size, heads, names),
        out_shape=VMEM((size, model_width), BF16),
        in_specs=[hbm] * len(inputs),
        out_specs=pl.BlockSpec(memory_space=pltpu.VMEM),
        scratch_shapes=list(scratch.values()),
        compiler_params=pltpu.CompilerParams(
            collective_id=0, has_side_effects=True, vmem_limit_bytes=KERNEL_VMEM
        ),
    )(*(pltpu.with_memory_space_constraint(value, pltpu.HBM) for value in inputs.values()))


def solution(mesh):
    placed = (
        P("sp", "tp"),
        P(),
        P(None, "tp"),
        P(None, "tp"),
        P(None, "tp"),
        P(None, "tp"),
        P(None, "tp"),
        P(),
        P(),
        P(),
        P(None, "sp"),
        P(None, "sp"),
        P(None, "tp", None, None),
        P(None, "tp", None),
        P(None, "tp"),
        P(),
        P(),
        P(),
        P(),
        P(),
    )
    return jax.shard_map(
        per_device, mesh=mesh, in_specs=placed, out_specs=P(("sp", "tp"), None), check_vma=False
    )
```

```python
import contextlib
import functools
import types

import jax
import jax.numpy as jnp
from jax import lax
from jax.experimental import pallas as pl
from jax.experimental.pallas import tpu as pltpu
from jax.sharding import PartitionSpec as P

DH = 128
NEG_BIG = -1e30
LN_EPS = 1e-05
HEAD_EPS = 1e-06
RIM = 16
AUG = 144
VMEM = pltpu.VMEM
MESH = pl.DeviceIdType.MESH
F32 = jnp.float32
BF16 = jnp.bfloat16
PROFILE = False
KERNEL_VMEM = 48 * 1024 * 1024
SMALL = (
    "gin", "gfg", "gain", "scale", "extra", "bias", "start_mem", "start_norm", "start_log",
    "map", "pscale", "hgain",
)


def scope(name):
    return jax.named_scope(name) if PROFILE else contextlib.nullcontext()


def scan_lanes(values, combine, neutral, forward_rows):
    lanes = values.shape[1]
    lane = lax.broadcasted_iota(jnp.int32, values.shape, 1)
    forward = lax.broadcasted_iota(jnp.int32, values.shape, 0) < forward_rows
    shift = 1
    while shift < lanes:
        low = jnp.where(lane >= shift, pltpu.roll(values, shift, 1), neutral)
        high = jnp.where(lane < lanes - shift, pltpu.roll(values, lanes - shift, 1), neutral)
        values = combine(values, jnp.where(forward, low, high))
        shift *= 2
    return values


def split_three(values):
    high = values.astype(BF16)
    rest = values - high.astype(F32)
    middle = rest.astype(BF16)
    low = (rest - middle.astype(F32)).astype(BF16)
    return high.astype(F32), middle.astype(F32), low.astype(F32)


def wide(row, lanes):
    return jnp.concatenate([row] * (lanes // row.shape[1]), axis=1)


def layer_kernel(tp_size, sp_size, heads, names, *refs):
    k = types.SimpleNamespace(**dict(zip(names, refs, strict=True)))
    me = lax.axis_index("sp")
    group = lax.axis_index("tp")
    far = lax.rem(group + tp_size // 2, tp_size)
    near = group + 1 - 2 * lax.rem(group, 2)
    diagonal = lax.rem(near + tp_size // 2, tp_size)
    others = (far, diagonal, near)
    rows_total, width = k.tokens.shape
    small_refs = [(getattr(k, name + "_in"), getattr(k, name)) for name in SMALL]
    model_width = width * tp_size
    blocks = tp_size
    size = rows_total // blocks
    half = size // 2
    pairs = 2 * heads
    all_heads = k.gin.shape[1]
    group_dim = k.map.shape[1]
    mem_width = heads * DH
    last = blocks - 1
    odd = lax.rem(me, 2)
    partner = me + 1 - 2 * odd
    strides = [1]
    while strides[-1] * 2 < sp_size:
        strides.append(strides[-1] * 2)
    levels = len(strides)

    def route(level, r):
        stride = strides[level]
        if level == 0:
            return True, partner, True
        step = stride * (1 - 2 * r)
        target, source = me + step, me - step
        okay = jnp.logical_and(target >= 0, target < sp_size)
        has = jnp.logical_and(source >= 0, source < sp_size)
        return okay, target, has

    late_half = (me >= sp_size // 2).astype(jnp.int32)
    leading = (late_half, 1 - late_half)

    def when(condition):
        if condition is True:
            return lambda body: body()
        return pl.when(condition)

    rim_sends = (me + 1 < sp_size, me >= 1)
    rim_recvs = (me >= 1, me + 1 < sp_size)

    barrier = pltpu.get_barrier_semaphore()
    peers = jnp.int32(len(others))
    for other in others:
        pl.semaphore_signal(barrier, inc=1, device_id={"tp": other}, device_id_type=MESH)
    greets = []
    for stride in strides:
        greets += [(me + stride < sp_size, me + stride), (me >= stride, me - stride)]
    for okay, other in greets:
        peers = peers + okay.astype(jnp.int32)

        @pl.when(okay)
        def _():
            pl.semaphore_signal(barrier, inc=1, device_id={"sp": other}, device_id_type=MESH)

    spans = [(b * size, size) for b in range(last)]
    spans += [(last * size, half), (last * size + half, half)]
    token_loads = [
        pltpu.make_async_copy(k.tokens.at[pl.ds(a, n)], k.own.at[pl.ds(a, n)], k.token_sem.at[i])
        for i, (a, n) in enumerate(((0, size), (size, rows_total - size)))
    ]
    for load in token_loads:
        load.start()

    def load_all(pairs_of, semaphore):
        for source, target in pairs_of:
            pltpu.make_async_copy(source, target, semaphore).start()

    def wait_for(ref, semaphore):
        pltpu.make_async_copy(ref, ref, semaphore).wait()

    def own_rows(ref, r):
        mine = ref[r, 0:heads, :].astype(F32)
        for other in range(1, tp_size):
            mine = jnp.where(
                group == other, ref[r, other * heads : (other + 1) * heads, :].astype(F32), mine
            )
        return mine

    with scope("barrier"):
        pl.semaphore_wait(barrier, peers)

    def to_tp(source, target, send, recv, other):
        return pltpu.make_async_remote_copy(
            src_ref=source, dst_ref=target, send_sem=send, recv_sem=recv,
            device_id={"tp": other}, device_id_type=MESH,
        )

    def to_sp(source, target, send, recv, other):
        return pltpu.make_async_remote_copy(
            src_ref=source, dst_ref=target, send_sem=send, recv_sem=recv,
            device_id={"sp": other}, device_id_type=MESH,
        )

    to_far, onward = [], []
    to_near = to_tp(k.own, k.held.at[0], k.tp_send, k.near_recv, near)
    for i, (a, n) in enumerate(spans):
        s = pl.ds(a, n)
        to_far.append(to_tp(k.own.at[s], k.held.at[1, s], k.tp_send, k.far_recv.at[i], far))
        onward.append(
            to_tp(k.held.at[1, s], k.held.at[2, s], k.tp_send, k.pass_recv.at[i], near)
        )
    token_loads[0].wait()
    to_far[0].start()
    token_loads[1].wait()
    for copy in to_far[1:]:
        copy.start()
    to_near.start()
    smalls = [
        pltpu.make_async_copy(source, target, k.small_sem.at[i])
        for i, (source, target) in enumerate(small_refs)
    ]
    for load in smalls:
        load.start()
    pool_weight = pltpu.make_async_copy(
        k.wp_hbm, k.wpg.at[:, pl.ds(0, group_dim)], k.load_sem.at[0]
    )
    pool_weight.start()
    wk, wv, wq, wo = (k.weights.at[i] for i in range(4))
    load_all(
        ((k.wk_hbm, wk), (k.wv_hbm, wv), (k.wq_hbm, wq), (k.wo_hbm, wo)), k.load_sem.at[1]
    )

    mem_rows = [
        (k.wmo_hbm.at[pl.ds((g * heads + h) * DH, DH)], k.wmo.at[h, pl.ds(g * DH, DH)])
        for h in range(heads)
        for g in range(tp_size)
    ]
    out_weight = pltpu.make_async_copy(k.wpo_hbm, k.wpo, k.load_sem.at[2])
    out_weight.start()
    load_all(mem_rows, k.load_sem.at[3])
    for load in smalls:
        load.wait()

    bias_lane = lax.broadcasted_iota(jnp.int32, k.bias.shape, 1)
    picked = [
        jnp.sum(jnp.where(bias_lane == group * heads + h, k.bias[...], 0.0), axis=1, keepdims=True)
        for h in range(heads)
    ]
    bias = jnp.concatenate([picked[h][r : r + 1] for r in range(2) for h in range(heads)], axis=0)

    s_at = lax.broadcasted_iota(jnp.int32, (size, size), 0)
    t_at = lax.broadcasted_iota(jnp.int32, (size, size), 1)

    def gate_weights():
        gate_rows = jnp.concatenate([own_rows(ref, r) for ref in (k.gin, k.gfg) for r in range(2)], axis=0)
        gate_rows = jnp.concatenate(
            [gate_rows, jnp.zeros((128 - 2 * pairs, model_width), F32)], axis=0
        )
        for n in range(model_width // 128):
            at = slice(n * 128, (n + 1) * 128)
            k.wpg[at, group_dim : group_dim + 128] = jnp.transpose(gate_rows[:, at]).astype(BF16)
        k.sums[:, 0:size] = (s_at <= t_at).astype(F32).astype(BF16)
        k.sums[:, size : 2 * size] = (s_at >= t_at).astype(F32).astype(BF16)

    def both_rows(ref, span):
        return jnp.concatenate(
            [jnp.broadcast_to(ref[r : r + 1, span], (heads, size)) for r in range(2)], axis=0
        )

    def add_sums(sums, view):
        part = view.astype(F32)
        return (
            sums[0] + jnp.sum(part, axis=1, keepdims=True),
            sums[1] + jnp.sum(part * part, axis=1, keepdims=True),
        )

    def early_sums(a, n):
        rows = slice(a, a + n)
        sums = (jnp.zeros((n, 1), F32), jnp.zeros((n, 1), F32))
        for view in (k.own[rows, :], k.held[0, rows, :], k.held[1, rows, :]):
            sums = add_sums(sums, view)
        return sums

    def normalize(a, n, at, sums):
        rows = slice(a, a + n)
        views = [k.own[rows, :]] + [k.held[slot, rows, :] for slot in range(3)]
        total, square = add_sums(sums, views[3])
        mean = total / model_width
        inverse = lax.rsqrt(square / model_width - mean * mean + LN_EPS)
        for view, owner in zip(views, (group, near, far, diagonal)):
            columns = pl.ds(pl.multiple_of(owner * width, width), width)
            k.normed[at : at + n, columns] = (
                (view.astype(F32) - mean) * inverse * k.gain[:, columns]
            ).astype(BF16)

    def project(a, n, at, targets):
        x = k.normed[at : at + n, :]
        for weight, target in targets:
            target[a : a + n, :] = jnp.dot(x, weight[...], preferred_element_type=F32).astype(BF16)

    def project_gates(a, n, at):
        x = k.normed[at : at + n, :]
        mixed = jnp.dot(x, k.wpg[...], preferred_element_type=F32)
        k.ext[RIM + a : RIM + a + n, :] = mixed[:, :group_dim].astype(BF16).astype(F32)
        k.gates[:, at : at + n] = jnp.transpose(mixed[:, group_dim:])[: 2 * pairs]

    zero_state = jnp.zeros((AUG, DH), F32)

    def initial(r, h):
        is_first = me == (0 if r == 0 else sp_size - 1)
        begin = jnp.broadcast_to(k.start_log[r : r + 1, h : h + 1], (1, 128))
        level = jnp.where(is_first, begin, NEG_BIG)
        rows = jnp.concatenate(
            [k.start_mem[r, h], jnp.broadcast_to(k.start_norm[r, h : h + 1, :], (AUG - DH, DH))], axis=0
        )
        return jnp.where(is_first, rows, 0.0), level

    def prepare():
        for h in range(heads):
            state, level = initial(0, h)
            k.cur_t[h] = state
            k.cur_s[h : h + 1, :] = level
            k.cur_t[heads + h] = zero_state
            k.cur_s[heads + h : heads + h + 1, :] = jnp.full((1, 128), NEG_BIG, F32)
        k.cur_s[pairs : 2 * pairs, :] = jnp.zeros((pairs, 128), F32)

    def summary(b):
        span = slice(b * size, (b + 1) * size)
        pre = k.gates[pairs : 2 * pairs, :] + bias
        log_sig = jnp.minimum(pre, 0.0) - jnp.log1p(jnp.exp(-jnp.abs(pre)))
        log_fg = log_sig * both_rows(k.scale, span) + both_rows(k.extra, span)
        parts = jnp.concatenate(split_three(log_fg), axis=0).astype(BF16)
        sums = jnp.dot(parts, k.sums[...], preferred_element_type=F32)
        sums = sums[:pairs] + sums[pairs : 2 * pairs] + sums[2 * pairs :]
        falls = jnp.concatenate([sums[:heads, :size], sums[heads:, size:]], axis=0)
        lifted = k.gates[:pairs, :] - falls
        top = jnp.max(lifted, axis=1, keepdims=True)
        sources = lifted + jnp.log(F32(DH ** -0.5))
        k.lifted[...] = lifted
        weights = jnp.exp(sources - top)
        peaks = jnp.broadcast_to(top, (pairs, 128))
        fall = jnp.concatenate(
            [falls[:heads, size - 1 : size], falls[heads:, 0:1]], axis=0
        )
        fall = jnp.broadcast_to(fall, (pairs, 128))
        for h in range(heads):
            cols = slice(h * DH, (h + 1) * DH)
            keys = k.k[span, cols]
            vt = jnp.concatenate(
                [jnp.transpose(k.v[span, cols].astype(F32)), jnp.ones((AUG - DH, size), F32)], axis=0
            )
            k.vt[h] = vt.astype(BF16)
            adds = [
                jnp.dot(
                    (vt * weights[p : p + 1]).astype(BF16), keys, preferred_element_type=F32
                )
                for p in (h, heads + h)
            ]
            p = h
            peak, down = peaks[p : p + 1], fall[p : p + 1]
            level = k.cur_s[p : p + 1, :]
            k.enter_t[0, h] = k.cur_t[p].astype(BF16)
            k.enter_s[0, h : h + 1, :] = level
            k.fcum[b, p : p + 1, :] = k.cur_s[pairs + p : pairs + p + 1, :]
            joint = jnp.maximum(level, peak)
            k.cur_t[p] = jnp.exp(level - joint) * k.cur_t[p] + jnp.exp(peak - joint) * adds[0]
            k.cur_s[p : p + 1, :] = joint + down
            k.cur_s[pairs + p : pairs + p + 1, :] += down
            p = heads + h
            peak, down = peaks[p : p + 1], fall[p : p + 1]
            k.ends[b, p : p + 1, :] = peak
            k.ends[b, pairs + p : pairs + p + 1, :] = down
            late = k.cur_s[p : p + 1, :]
            late_fall = k.cur_s[pairs + p : pairs + p + 1, :]
            if b < last:
                k.adds[h, b] = adds[1]
                early, level = adds[1], peak + down
            else:
                state, level = initial(1, h)
                k.back_t[h, b] = state.astype(BF16)
                k.back_s[b, h : h + 1, :] = level
                joint = jnp.maximum(level, peak)
                early = jnp.exp(level - joint) * state + jnp.exp(peak - joint) * adds[1]
                level = joint + down
                if b > 0:
                    k.back_f[h] = early
                    k.back_s[b - 1, h : h + 1, :] = level
            level = level + late_fall
            joint = jnp.maximum(level, late)
            k.cur_t[p] = jnp.exp(level - joint) * early + jnp.exp(late - joint) * k.cur_t[p]
            k.cur_s[p : p + 1, :] = joint
            k.cur_s[pairs + p : pairs + p + 1, :] = late_fall + down

    def local_block(b):
        span = slice(b * size, (b + 1) * size)
        lifted = k.lifted[...]
        peaks = scan_lanes(lifted, jnp.maximum, NEG_BIG, heads)
        levels_in = jnp.concatenate(
            [wide(k.enter_s[0, 0:heads, :], size), jnp.full((heads, size), NEG_BIG, F32)], axis=0
        )
        peaks = jnp.maximum(peaks, levels_in)
        k.peaks[b, 0:pairs, :] = peaks
        carry = jnp.exp(levels_in[:heads] - peaks[:heads])
        sources = lifted + jnp.log(F32(DH ** -0.5))
        columns = jnp.transpose(
            jnp.concatenate([sources, jnp.zeros((128 - pairs, size), F32)], axis=0)
        )
        for h in range(heads):
            cols = slice(h * DH, (h + 1) * DH)
            queries = k.q[span, cols]
            scores = lax.dot_general(
                k.k[span, cols], queries, (((1,), (1,)), ((), ())), preferred_element_type=F32
            )
            values = k.vt[h]
            before = lax.dot_general(
                k.enter_t[0, h], queries, (((1,), (1,)), ((), ())), preferred_element_type=F32
            )
            for r in range(2):
                p = r * heads + h
                inside = (s_at <= t_at) if r == 0 else (s_at >= t_at)
                weight = jnp.exp(
                    jnp.where(inside, columns[:, p : p + 1] - peaks[p : p + 1], NEG_BIG)
                )
                result = jnp.dot(
                    values, (scores * weight).astype(BF16), preferred_element_type=F32
                )
                if r == 0:
                    result = result + carry[h : h + 1] * before
                k.locals[p, b] = result

    def out_gates(b):
        span = slice(b * size, (b + 1) * size)
        for h in range(heads):
            opened = jnp.transpose(k.o[span, h * DH : (h + 1) * DH].astype(F32))
            gain = k.hgain[:, pl.ds(pl.multiple_of(group * mem_width + h * DH, DH), DH)]
            column = jnp.transpose(jnp.broadcast_to(gain, (128, DH)))
            k.gated[h, b] = wide(column, size) / (1.0 + jnp.exp(-opened))

    with scope("prepare"):
        gate_weights()
        prepare()
    def rim(side):
        other = me + 1 if side == 0 else me - 1
        return to_sp(k.rim_out.at[side], k.rims.at[side], k.rs.at[side], k.rr.at[side], other)

    def start_rims():
        k.rim_out[1] = k.ext[RIM : 2 * RIM, :].astype(BF16)
        k.rim_out[0] = k.ext[rows_total : RIM + rows_total, :].astype(BF16)
        for side in range(2):
            @pl.when(rim_sends[side])
            def _():
                rim(side).start()

    def pass_on(i):
        to_far[i].wait_recv()
        onward[i].start()

    for b in range(blocks):
        pieces = [i for i, (a, n) in enumerate(spans) if b * size <= a < (b + 1) * size]
        with scope(f"far{b}"):
            for i in pieces[1 if b == last and b > 0 else 0 :]:
                pass_on(i)
        for i in pieces:
            a, n = spans[i]
            at = a - b * size
            if i == 0:
                to_near.wait_recv()
            with scope(f"wait{i}"):
                sums = early_sums(a, n)
                onward[i].wait_recv()
            if i == 0:
                pool_weight.wait()
                wait_for(k.weights, k.load_sem.at[1])
            with scope(f"project{i}"):
                normalize(a, n, at, sums)
                project_gates(a, n, at)
                project(a, n, at, ((wk, k.k), (wv, k.v)))
        if b == last - 1:
            with scope("far_half"):
                pass_on(last)
        if b < last:
            with scope(f"local{b}"):
                project(b * size, size, 0, ((wq, k.q), (wo, k.o)))
                summary(b)
                local_block(b)
                out_gates(b)
        else:
            with scope(f"summary{b}"):
                start_rims()
                summary(b)

    for r in range(2):
        for h in range(heads):
            p = r * heads + h
            k.inc_s[r, h : h + 1, :] = k.cur_s[p : p + 1, :]
            k.inc_s[r, heads + h : heads + h + 1, :] = k.cur_s[pairs + p : pairs + p + 1, :]

    def scalar_copy(level, r):
        return to_sp(
            k.send_s.at[level, r], k.recv_s.at[level, r], k.ss.at[level, r], k.sr.at[level, r],
            route(level, r)[1],
        )

    def state_copy(level, r, h):
        return to_sp(
            k.send_t.at[level, r, h], k.recv_t.at[level, r, h], k.ts.at[level, r],
            k.tr.at[level, r, h], route(level, r)[1],
        )

    def ready(slot, level, r):
        okay = route(level, r)[0]
        if slot >= 2:
            okay = jnp.logical_and(okay, route(slot - 1, r)[2])
        if level > slot:
            okay = jnp.logical_and(okay, jnp.logical_not(route(slot, r)[2]))
        return okay

    def send_scalars(slot):
        for r in range(2):
            for level in range(slot, levels if slot > 0 else 1):
                @when(ready(slot, level, r))
                def _():
                    k.send_s[level, r] = k.inc_s[r]
                    scalar_copy(level, r).start()

    def send_state(slot, r, h):
        for level in range(slot, levels if slot > 0 else 1):
            @when(ready(slot, level, r))
            def _():
                k.send_t[level, r, h] = k.cur_t[r * heads + h].astype(BF16)
                state_copy(level, r, h).start()

    def take_scalars(level):
        for r in range(2):
            @when(route(level, r)[2])
            def _():
                scalar_copy(level, r).wait_recv()
                theirs_max = k.recv_s[level, r, 0:heads, :]
                theirs_fall = k.recv_s[level, r, heads : 2 * heads, :]
                own_max = k.inc_s[r, 0:heads, :]
                own_fall = k.inc_s[r, heads : 2 * heads, :]
                if level == 0:
                    early = (odd == 1) if r == 0 else (odd == 0)
                    a = jnp.where(early, theirs_max + own_fall, theirs_max)
                    c = jnp.where(early, own_max, own_max + theirs_fall)
                    flag = jnp.where(early, 1.0, 0.0).astype(F32)
                    k.weigh[r, 2 * heads : 3 * heads, :] = jnp.full((heads, 128), flag, F32)
                    k.exc_s[r, 0:heads, :] = jnp.where(early, theirs_max, NEG_BIG)
                    k.exc_s[r, heads : 2 * heads, :] = jnp.where(early, theirs_fall, 0.0)
                else:
                    a = theirs_max + own_fall
                    c = own_max
                    late_max = k.exc_s[r, 0:heads, :]
                    late_fall = k.exc_s[r, heads : 2 * heads, :]
                    level_in = theirs_max + late_fall
                    top = jnp.maximum(level_in, late_max)
                    k.weigh[r, 2 * heads : 3 * heads, :] = jnp.exp(level_in - top)
                    k.weigh[r, 3 * heads : 4 * heads, :] = jnp.exp(late_max - top)
                    k.exc_s[r, 0:heads, :] = top
                    k.exc_s[r, heads : 2 * heads, :] = theirs_fall + late_fall
                top = jnp.maximum(a, c)
                k.weigh[r, 0:heads, :] = jnp.exp(a - top)
                k.weigh[r, heads : 2 * heads, :] = jnp.exp(c - top)
                k.inc_s[r, 0:heads, :] = top
                k.inc_s[r, heads : 2 * heads, :] = theirs_fall + own_fall

    def take_state(level, r, h):
        @when(route(level, r)[2])
        def _():
            state_copy(level, r, h).wait_recv()
            p = r * heads + h
            arrived = k.recv_t[level, r, h].astype(F32)
            if level + 1 < levels:
                k.cur_t[p] = (
                    k.weigh[r, h : h + 1, :] * arrived
                    + k.weigh[r, heads + h : heads + h + 1, :] * k.cur_t[p]
                )
            mine = k.weigh[r, 2 * heads + h : 2 * heads + h + 1, :] * arrived
            if level > 0:
                mine = mine + k.weigh[r, 3 * heads + h : 3 * heads + h + 1, :] * k.exc_t[p]
            k.exc_t[p] = mine

    def pooling():
        for side in range(2):
            at = 0 if side == 0 else RIM + rows_total

            @pl.when(rim_recvs[side])
            def _():
                rim(side).wait_recv()
                k.ext[at : at + RIM, :] = k.rims[side].astype(F32)

            @pl.when(jnp.logical_not(rim_recvs[side]))
            def _():
                k.ext[at : at + RIM, :] = jnp.zeros((RIM, group_dim), F32)
        half_span = jnp.left_shift(jnp.int32(1), group)
        for n in range(blocks):
            first = n * size
            chunk = k.ext[first : first + size + 2 * RIM, :]
            own = chunk[RIM : RIM + size]
            low = 1
            running = chunk[: size + 2 * RIM - 1] + chunk[1:]
            reach = 1
            while 2 * reach < RIM:
                span = running.shape[0] - 2 * reach
                longer = running[:span] + running[2 * reach :]
                kept = running[reach : reach + span]
                running = jnp.where(half_span > reach, longer, kept)
                low += reach
                reach *= 2
            pooled = running[RIM - low : RIM - low + size]
            position = me * rows_total + first + lax.broadcasted_iota(jnp.int32, own.shape, 0)
            count = jnp.minimum(position + half_span, rows_total * sp_size) - jnp.maximum(
                position - half_span, 0
            )
            contrast = (pooled / count.astype(F32) - own).astype(BF16)
            mapped = jnp.dot(contrast, k.map[group], preferred_element_type=F32)
            scale = k.pscale[:, pl.ds(pl.multiple_of(group * group_dim, group_dim), group_dim)]
            k.pool_out[first : first + size, :] = (mapped * scale).astype(BF16)

    pool_cols = pl.ds(pl.multiple_of(group * group_dim, group_dim), group_dim)

    def rows_of(owner):
        return pl.ds(pl.multiple_of(owner * size, size), size)

    own_cols = pl.ds(pl.multiple_of(group * DH, DH), DH)

    pool_copies = [
        to_tp(k.pool_out.at[rows_of(other)], k.lhs_pool.at[:, pool_cols], k.pool_send, k.pr, other)
        for j, other in enumerate(others)
    ]
    mem_copies = [
        [
            to_tp(
                k.mem_out.at[h, rows_of(other)], k.lhs_mem.at[h, :, own_cols],
                k.mem_send, k.mr.at[h] if j < 2 else k.mn.at[h], other,
            )
            for j, other in enumerate(others)
        ]
        for h in range(heads)
    ]

    def start_pool():
        pooling()
        for copy in pool_copies:
            copy.start()

    home = pl.ds(pl.multiple_of(lax.div(group, 2) * 2 * DH, 2 * DH), 2 * DH)
    away = pl.ds(pl.multiple_of(lax.div(far, 2) * 2 * DH, 2 * DH), 2 * DH)
    tile = 512

    def mem_product(h, span, cols):
        return jnp.dot(k.lhs_mem[h, :, span], k.wmo[h, span, cols], preferred_element_type=F32)

    def home_product():
        k.lhs_pool[:, pool_cols] = k.pool_out[rows_of(group), :]
        wait_for(k.pool_out.at[pl.ds(0, len(others) * size)], k.pr)
        out_weight.wait()
        wait_for(k.wmo, k.load_sem.at[3])
        for h in range(heads):
            wait_for(k.mem_out.at[h, pl.ds(0, size)], k.mn.at[h])
        for n in range(model_width // tile):
            cols = slice(n * tile, (n + 1) * tile)
            total = jnp.dot(k.lhs_pool[...], k.wpo[:, cols], preferred_element_type=F32)
            for h in range(heads):
                total = total + mem_product(h, home, cols)
            k.acc[:, cols] = total

    def last_local():
        project(last * size, size, 0, ((wq, k.q), (wo, k.o)))
        local_block(last)
        out_gates(last)

    def backward_enter():
        for h in range(heads):
            p = heads + h
            fall = k.ends[last, pairs + p : pairs + p + 1, :]
            k.fcum[last, p : p + 1, :] = jnp.zeros((1, 128), F32)
            if blocks > 1:
                state, level = k.back_f[h], k.back_s[last - 1, h : h + 1, :]
            for b in reversed(range(last)):
                k.back_t[h, b] = state.astype(BF16)
                k.fcum[b, p : p + 1, :] = fall
                if b > 0:
                    peak = k.ends[b, p : p + 1, :]
                    down = k.ends[b, pairs + p : pairs + p + 1, :]
                    joint = jnp.maximum(level, peak)
                    state = jnp.exp(level - joint) * state + jnp.exp(peak - joint) * k.adds[h, b]
                    level = joint + down
                    k.back_s[b - 1, h : h + 1, :] = level
                    fall = fall + down
        for b in range(blocks):
            span = slice(b * size, (b + 1) * size)
            for h in range(heads):
                p = heads + h
                level = wide(k.back_s[b, h : h + 1, :], size)
                peak = k.peaks[b, p : p + 1, :]
                joint = jnp.maximum(level, peak)
                before = lax.dot_general(
                    k.back_t[h, b], k.q[span, h * DH : (h + 1) * DH], (((1,), (1,)), ((), ())),
                    preferred_element_type=F32,
                )
                k.locals[p, b] = (
                    jnp.exp(peak - joint) * k.locals[p, b] + jnp.exp(level - joint) * before
                )
                k.peaks[b, p : p + 1, :] = joint

    def finish(b, h):
        states = jnp.concatenate([k.exc_t[h], k.exc_t[heads + h]], axis=0).astype(BF16)
        queries = k.q[rows_of(b), h * DH : (h + 1) * DH]
        entered = lax.dot_general(
            states, queries, (((1,), (1,)), ((), ())), preferred_element_type=F32
        )
        hidden = None
        for r in range(2):
            p = r * heads + h
            level = wide(k.exc_s[r, h : h + 1, :] + k.fcum[b, p : p + 1, :], size)
            peak = k.peaks[b, p : p + 1, :]
            joint = jnp.maximum(level, peak)
            a = jnp.exp(peak - joint)
            c = jnp.exp(level - joint)
            mine = k.locals[p, b]
            theirs = entered[r * AUG : (r + 1) * AUG]
            below = a * mine[DH : DH + 1] + c * theirs[DH : DH + 1]
            inverse = 1.0 / jnp.maximum(jnp.abs(below), 1.0)
            part = (a * inverse) * mine[:DH] + (c * inverse) * theirs[:DH]
            hidden = part if hidden is None else hidden + part
        centered = hidden - jnp.mean(hidden, axis=0, keepdims=True)
        variance = jnp.mean(centered * centered, axis=0, keepdims=True)
        scaled = centered * lax.rsqrt(variance + HEAD_EPS) * k.gated[h, b]
        return jnp.transpose(scaled).astype(BF16)

    with scope("send0"):
        send_scalars(0)
        for h in range(heads):
            for r in leading:
                send_state(0, r, h)
        wait_for(k.held, k.tp_send)
    for r in range(2):
        for h in range(heads):
            k.exc_t[r * heads + h] = zero_state
    with scope("last_local"):
        last_local()

    def settle(level, directions=(0, 1)):
        for r in directions:
            @when(route(level, r)[0])
            def _():
                scalar_copy(level, r).wait_send()
                wait_for(k.send_t.at[level, r], k.ts.at[level, r])

    for level in range(levels):
        final = level + 1 == levels
        if final:
            if level == 0:
                start_pool()
            with scope("backward_enter"):
                backward_enter()
        with scope(f"scalars{level}"):
            take_scalars(level)
            if not final:
                send_scalars(level + 1)
        for h in range(heads):
            with scope(f"states{level}_{h}"):
                for r in leading:
                    take_state(level, r, h)
                    if not final:
                        send_state(level + 1, r, h)
            if final:
                with scope(f"finish{h}"):
                    for j in range(2):
                        k.mem_out[h, rows_of(others[j])] = finish(others[j], h)
                        mem_copies[h][j].start()
                        if h == 0:
                            settle(0, (j,))
                        elif h == 1 and j == 0:
                            wait_for(k.pool_out.at[pl.ds(0, len(others) * size)], k.pool_send)
                with scope(f"finish_near{h}"):
                    k.mem_out[h, rows_of(near)] = finish(near, h)
                    mem_copies[h][2].start()
                with scope(f"finish_own{h}"):
                    k.lhs_mem[h, :, own_cols] = finish(group, h)
            elif level == 0 and h == 0:
                with scope("pooling"):
                    start_pool()
    with scope("home_product"):
        home_product()
    for h in range(heads):
        with scope(f"wait_mem{h}"):
            wait_for(k.mem_out.at[h, pl.ds(0, 2 * size)], k.mr.at[h])
        with scope(f"product{h}"):
            for n in range(model_width // tile):
                cols = slice(n * tile, (n + 1) * tile)
                total = k.acc[:, cols] + mem_product(h, away, cols)
                if h + 1 < heads:
                    k.acc[:, cols] = total
                else:
                    k.out[:, cols] = total.astype(BF16)

    with scope("leave"):
        if heads < 2:
            wait_for(k.pool_out.at[pl.ds(0, len(others) * size)], k.pool_send)
        wait_for(k.mem_out.at[:, pl.ds(0, len(others) * size)], k.mem_send)
        for level in range(1, levels):
            settle(level)
        for side in range(2):
            @pl.when(rim_sends[side])
            def _():
                rim(side).wait_send()


def per_device(
    tokens,
    input_norm_gain,
    pooling_input_matrix,
    query_projection_matrix,
    key_projection_matrix,
    value_projection_matrix,
    output_gate_matrix,
    input_gate_matrix,
    forget_gate_matrix,
    forget_gate_bias,
    log_forget_scale,
    extra_log_forget,
    starting_memory,
    starting_normalizer,
    starting_log_scale,
    pooling_group_map,
    pooling_channel_scale,
    memory_head_gain,
    pooling_output_matrix,
    memory_output_matrix,
):
    rows, own_width = tokens.shape
    tp_size = lax.axis_size("tp")
    sp_size = lax.axis_size("sp")
    model_width = own_width * tp_size
    group_dim = pooling_input_matrix.shape[1]
    heads = query_projection_matrix.shape[1] // DH
    mem_width = heads * DH
    pairs = 2 * heads
    levels = max(1, (sp_size - 1).bit_length())
    blocks = tp_size
    size = rows // blocks
    pool_total = pooling_output_matrix.shape[0]
    mem_total = memory_output_matrix.shape[0]
    hbm = pl.BlockSpec(memory_space=pltpu.HBM)
    dma = pltpu.SemaphoreType.DMA
    small = dict(
        gin=input_gate_matrix.transpose(1, 2, 0),
        gfg=forget_gate_matrix.transpose(1, 2, 0),
        gain=input_norm_gain.reshape(1, model_width),
        scale=log_forget_scale,
        extra=extra_log_forget,
        bias=forget_gate_bias,
        start_mem=starting_memory,
        start_norm=starting_normalizer,
        start_log=starting_log_scale,
        map=pooling_group_map,
        pscale=pooling_channel_scale.reshape(1, pool_total),
        hgain=memory_head_gain.reshape(1, mem_total),
    )
    inputs = dict(
        tokens=tokens,
        **{name + "_in": small[name] for name in SMALL},
        wp_hbm=pooling_input_matrix,
        wq_hbm=query_projection_matrix,
        wk_hbm=key_projection_matrix,
        wv_hbm=value_projection_matrix,
        wo_hbm=output_gate_matrix,
        wpo_hbm=pooling_output_matrix,
        wmo_hbm=memory_output_matrix,
    )
    scratch = dict(
        **{name: VMEM(small[name].shape, small[name].dtype) for name in SMALL},
        own=VMEM((rows, own_width), BF16),
        held=VMEM((3, rows, own_width), BF16),
        normed=VMEM((size, model_width), BF16),
        wpg=VMEM((model_width, group_dim + 128), BF16),
        weights=VMEM((4, model_width, mem_width), BF16),
        wpo=VMEM((pool_total, model_width), BF16),
        wmo=VMEM((heads, tp_size * DH, model_width), BF16),
        lhs_mem=VMEM((heads, size, tp_size * DH), BF16),
        acc=VMEM((size, model_width), F32),
        sums=VMEM((size, 2 * size), BF16),
        ext=VMEM((rows + 2 * RIM, group_dim), F32),
        q=VMEM((rows, mem_width), BF16),
        k=VMEM((rows, mem_width), BF16),
        v=VMEM((rows, mem_width), BF16),
        o=VMEM((rows, mem_width), BF16),
        gates=VMEM((2 * pairs, size), F32),
        lifted=VMEM((pairs, size), F32),
        vt=VMEM((heads, AUG, size), BF16),
        adds=VMEM((heads, blocks, AUG, DH), F32),
        ends=VMEM((blocks, 2 * pairs, 128), F32),
        fcum=VMEM((blocks, pairs, 128), F32),
        peaks=VMEM((blocks, pairs, size), F32),
        locals=VMEM((pairs, blocks, AUG, size), F32),
        gated=VMEM((heads, blocks, DH, size), F32),
        cur_t=VMEM((pairs, AUG, DH), F32),
        cur_s=VMEM((2 * pairs, 128), F32),
        enter_t=VMEM((1, heads, AUG, DH), BF16),
        enter_s=VMEM((1, heads, 128), F32),
        back_t=VMEM((heads, blocks, AUG, DH), BF16),
        back_f=VMEM((heads, AUG, DH), F32),
        back_s=VMEM((blocks, heads, 128), F32),
        inc_s=VMEM((2, 2 * heads, 128), F32),
        exc_t=VMEM((pairs, AUG, DH), F32),
        exc_s=VMEM((2, 2 * heads, 128), F32),
        weigh=VMEM((2, 4 * heads, 128), F32),
        send_t=VMEM((levels, 2, heads, AUG, DH), BF16),
        send_s=VMEM((levels, 2, 2 * heads, 128), F32),
        recv_t=VMEM((levels, 2, heads, AUG, DH), BF16),
        recv_s=VMEM((levels, 2, 2 * heads, 128), F32),
        rim_out=VMEM((2, RIM, group_dim), BF16),
        rims=VMEM((2, RIM, group_dim), BF16),
        pool_out=VMEM((rows, group_dim), BF16),
        mem_out=VMEM((heads, rows, DH), BF16),
        lhs_pool=VMEM((size, pool_total), BF16),
        token_sem=dma((2,)),
        small_sem=dma((len(SMALL),)),
        load_sem=dma((4,)),
        tp_send=dma,
        pool_send=dma,
        mem_send=dma,
        near_recv=dma,
        far_recv=dma((blocks + 1,)),
        pass_recv=dma((blocks + 1,)),
        ts=dma((levels, 2)),
        tr=dma((levels, 2, heads)),
        ss=dma((levels, 2)),
        sr=dma((levels, 2)),
        rs=dma((2,)),
        rr=dma((2,)),
        pr=dma,
        mr=dma((heads,)),
        mn=dma((heads,)),
    )
    names = tuple(inputs) + ("out",) + tuple(scratch)
    return pl.pallas_call(
        functools.partial(layer_kernel, tp_size, sp_size, heads, names),
        out_shape=VMEM((size, model_width), BF16),
        in_specs=[hbm] * len(inputs),
        out_specs=pl.BlockSpec(memory_space=pltpu.VMEM),
        scratch_shapes=list(scratch.values()),
        compiler_params=pltpu.CompilerParams(
            collective_id=0, has_side_effects=True, vmem_limit_bytes=KERNEL_VMEM
        ),
    )(*(pltpu.with_memory_space_constraint(value, pltpu.HBM) for value in inputs.values()))


def solution(mesh):
    placed = (
        P("sp", "tp"),
        P(),
        P(None, "tp"),
        P(None, "tp"),
        P(None, "tp"),
        P(None, "tp"),
        P(None, "tp"),
        P(),
        P(),
        P(),
        P(None, "sp"),
        P(None, "sp"),
        P(None, "tp", None, None),
        P(None, "tp", None),
        P(None, "tp"),
        P(),
        P(),
        P(),
        P(),
        P(),
    )
    return jax.shard_map(
        per_device, mesh=mesh, in_specs=placed, out_specs=P(("sp", "tp"), None), check_vma=False
    )
```
